512 devices in a mesh: sp: 32 (over z, x), tp: 16 (over y, core).
Axes of the slice: x: 4, y: 8, z: 8, core: 2. Of those that a mesh axis runs over, the one named last changes fastest.
Arguments:
- pool_input: bfloat16 [1024, 12288], P('tp', 'sp'), may hold values from -6 to 6
- pool_gate: bfloat16 [1024, 12288], P('tp', 'sp'), may hold values from -6 to 6
- pool_mix: bfloat16 [4, 256, 256], replicated, may hold values from -0.375 to 0.375
- pool_scale: float32 [1024], replicated, may hold values from 0.1 to 1.9
- out_proj: bfloat16 [1024, 2048], P(None, 'tp'), may hold values from -0.375 to 0.375
- residual: bfloat16 [12288, 2048], P('sp', 'tp'), may hold values from -12 to 12
- norm_gain: float32 [2048], P('tp'), may hold values from 0.1 to 1.9
- routes: int32 [12288, 2], P('sp'), may hold values from 0 to 31, all different within a row; in each aligned block of 384 rows (0 to 383, 384 to 767, ...) at most 36 rows name the same one
- group_logits: float32 [12288, 4], P('sp'), may hold values from -4 to 4
- expert_scores: float32 [12288, 2], P('sp'), may hold values from -4 to 4
- w_gate: bfloat16 [32, 2048, 4096], P('sp', None, 'tp'), may hold values from -0.125 to 0.125
- w_up: bfloat16 [32, 2048, 4096], P('sp', None, 'tp'), may hold values from -0.125 to 0.125
- w_down: bfloat16 [32, 4096, 2048], P('sp', None, 'tp'), may hold values from -0.375 to 0.375
Outputs:
- layer_out: bfloat16 [12288, 2048], P('sp', 'tp')
The draws below stay inside these ranges and needn't reach their ends.
Inputs may be any that keep to these rules, and one draw needn't show every extreme that they name: `routes`: among the rows of one device (aligned blocks of 384 rows) no expert is named by more than 36 rows, a bound that some block reaches; the 2 experts of a row differ.
All inputs are finite; a program needn't handle non-finite values.
Results may differ from the reference program's by a relative error of at most 0.01.
Values may be sent and summed in bfloat16 or wider, within the bound.
No kernel may reach another device: no remote copies, remote signals or barrier semaphores. Data moves between devices by JAX's collectives and lax.ppermute only.
A program may use at most 64 MiB of HBM per device.

```python
import math
import jax
import jax.numpy as jnp
import numpy as np
from jax import lax

D = 2048
POOL_WIDTH = 1024
POOL_GROUP = 256
FF = 4096
N_GROUPS = 4
TOP = 2
TOK_DEV = 384
EXPERTS = 32
CAP = 36
TOKENS = 12288
N_SP = 32


def draw_residual(key, part):
    columns = jnp.arange(D, dtype=jnp.float32)
    column_scale = jnp.exp(jnp.log(3.0) * columns / D)
    values = jnp.clip(jax.random.normal(key, (TOKENS, D), jnp.float32), -6.0, 6.0)
    drawn = values * column_scale[None, :] * 0.6
    return drawn.astype(jnp.bfloat16)


def levels(own_key, extent, shards, smallest, high):
    def one(dim, parts):
        steps = jax.random.uniform(jax.random.fold_in(jax.random.fold_in(own_key, 6), dim), (parts,), jnp.float32, smallest / len(shards), high / len(shards))
        return jnp.repeat(jnp.exp(steps), extent[dim] // parts).reshape((-1,) + (1,) * (len(extent) - dim - 1))

    loudness = one(*shards[0])
    for cut in shards[1:]:
        loudness = loudness * one(*cut)
    return loudness


def routed_block(key, own, number, rows, count, top, bound, slope):
    ranking = jax.random.permutation(key, count)
    packed, ordinary = load_shares(count, rows * top, bound, slope, True), load_shares(count, rows * top, bound, slope, False)
    places = jnp.arange(count)

    def named(tallies, rotation):
        used = int((tallies > 0).sum())
        fixed = max(1, used // 4)
        shifted = fixed + (places - fixed + rotation * (used - fixed)) % max(1, count - fixed)
        return jnp.zeros((count,), jnp.int32).at[ranking[jnp.where(places < fixed, places, shifted)]].set(jnp.asarray(tallies, jnp.int32))

    tallies = jnp.where(number % 4 == 0, named(packed, number // 4), named(ordinary, number - number // 4 - 1))
    mixed = jax.random.permutation(jax.random.fold_in(own, 3), count)
    giver, sink = mixed[0:count // 2 * 2:2], mixed[1:count // 2 * 2:2]
    margin = jnp.minimum(tallies[giver] - 1, bound - tallies[sink]) // 2
    margin = jnp.where((giver == ranking[0]) | (sink == ranking[0]) | (tallies[sink] == 0), 0, jnp.maximum(margin, 0))
    shifted = jax.random.randint(jax.random.fold_in(own, 4), (count // 2,), 0, 1 << 20) % (margin + 1)
    tallies = tallies.at[giver].add(-shifted).at[sink].add(shifted)
    members = jnp.searchsorted(jnp.cumsum(tallies), jnp.arange(rows * top), side="right").astype(jnp.int32)
    grid = members.reshape(top, rows).T
    grid = grid[jax.random.permutation(jax.random.fold_in(own, 1), rows)]
    rotation = jax.random.randint(jax.random.fold_in(own, 2), (rows, 1), 0, top)
    return jnp.take_along_axis(grid, (jnp.arange(top)[None, :] + rotation) % top, axis=1)


def load_shares(amount, total, reach, lean, full):
    portions = [(1 << 20) // math.isqrt(rank ** lean) + 1 for rank in range(1, amount + 1)]
    largest = reach if full else min(reach, max(-(-total // amount), total * portions[0] // sum(portions)))
    least = 1 if total - largest >= amount - 1 else 0
    holding, spare = [largest] + [least] * (amount - 1), total - largest - least * (amount - 1)
    while spare > 0:
        movable = [i for i in range(1, amount) if holding[i] < largest] or [i for i in range(1, amount) if holding[i] < reach]
        mass, budget = sum([portions[i] for i in movable]), spare
        for i in movable:
            more = min(reach - holding[i], max(1, budget * portions[i] // mass), spare)
            holding[i] = holding[i] + more
            spare = spare - more
    return np.array(holding)


def scatter_about(own_key, dims, deviation, bound, cuts=(), kind=jnp.bfloat16):
    values = jax.random.normal(own_key, dims, jnp.float32) * deviation
    if len(cuts) > 0:
        values = levels(own_key, dims, cuts, -0.22, 0.18) * values
    return jnp.clip(values, min=-bound, max=bound).astype(kind)


def setup_inputs(seed: int = 0) -> dict:
    seeds = jax.random.split(jax.random.key(seed), 14)
    pool_input = scatter_about(seeds[0], (POOL_WIDTH, TOKENS), 1.0, 6.0, ((0, 16), (1, 32)))
    pool_gate = scatter_about(seeds[1], (POOL_WIDTH, TOKENS), 1.5, 6.0, ((0, 16), (1, 32)))
    pool_mix = scatter_about(seeds[2], (4, POOL_GROUP, POOL_GROUP), POOL_GROUP ** -0.5, 0.375)
    pool_scale = jnp.clip(1.0 + 0.18 * jax.random.normal(seeds[3], (POOL_WIDTH,), jnp.float32), 0.1, 1.9)
    out_proj = scatter_about(seeds[4], (POOL_WIDTH, D), (POOL_WIDTH // 4) ** -0.5, 0.375, ((1, 16),))
    residual = draw_residual(jax.random.fold_in(seeds[13], 71), 0)
    norm_gain = jnp.clip(1.0 + 0.18 * jax.random.normal(seeds[6], (D,), jnp.float32), 0.1, 1.9)
    routes_keys = jax.random.split(jax.random.fold_in(seeds[7], 1), TOKENS // TOK_DEV)
    routes_turns = jax.random.permutation(jax.random.fold_in(seeds[7], 3), TOKENS // TOK_DEV)
    routes = jax.vmap(lambda own, number: routed_block(jax.random.fold_in(seeds[7], 2), own, number, TOK_DEV, EXPERTS, TOP, CAP, 2))(routes_keys, routes_turns).reshape((TOKENS, TOP))
    group_logits = scatter_about(seeds[8], (TOKENS, N_GROUPS), 1.0, 4.0, ((0, 32),), jnp.float32)
    expert_scores = scatter_about(seeds[9], (TOKENS, TOP), 1.0, 4.0, ((0, 32),), jnp.float32)
    w_gate = scatter_about(seeds[10], (EXPERTS, D, FF), D ** -0.5, 0.125, ((0, 32), (2, 16)))
    w_up = scatter_about(seeds[11], (EXPERTS, D, FF), D ** -0.5, 0.125, ((0, 32), (2, 16)))
    w_down = scatter_about(seeds[12], (EXPERTS, FF, D), (FF // 16) ** -0.5, 0.375, ((0, 32), (2, 16)))
    return dict(pool_input=pool_input, pool_gate=pool_gate, pool_mix=pool_mix, pool_scale=pool_scale, out_proj=out_proj, residual=residual, norm_gain=norm_gain, routes=routes, group_logits=group_logits, expert_scores=expert_scores, w_gate=w_gate, w_up=w_up, w_down=w_down)


reach_back = 15
epsilon = 1e-06

def window_terms(extended, first_channel, first_position, group_width):
    length = extended.shape[1] - reach_back
    layered = extended
    stride = 1
    partial_sums = []
    for _ in range(4):
        layered = layered[:, stride:] + layered[:, :-stride]
        stride = stride * 2
        partial_sums.append(layered[:, layered.shape[1] - length:])
    channel = first_channel + jnp.arange(extended.shape[0], dtype=jnp.int32)
    scale_index = channel // group_width
    chosen = partial_sums[3]
    for octave in range(3):
        chosen = jnp.where((scale_index == octave)[:, None], partial_sums[octave], chosen)
    window = (2 ** (scale_index + 1)).astype(jnp.float32)
    positions = (first_position + jnp.arange(length, dtype=jnp.int32) + 1).astype(jnp.float32)
    counted = jnp.minimum(positions[None, :], window[:, None])
    return chosen / counted - extended[:, reach_back:]

def slot_table(row_block, experts, capacity):
    flattened = row_block.reshape(-1)
    onehot = (flattened[:, None] == jnp.arange(experts, dtype=jnp.int32)[None, :]).astype(jnp.int32)
    before = jnp.cumsum(onehot, axis=0) - onehot
    ranked = lax.optimization_barrier(jnp.sum(before * onehot, axis=1))
    return flattened * capacity + ranked

def route_weights(routes, group_logits, expert_scores, per_group):
    raised = jnp.exp(group_logits)
    group_prob = raised / lax.optimization_barrier(jnp.sum(raised, axis=1, keepdims=True))
    owning_group = routes // per_group
    groups_iota = jnp.arange(group_logits.shape[1], dtype=jnp.int32)
    picked = lax.optimization_barrier(jnp.sum(jnp.where(owning_group[:, :, None] == groups_iota[None, None, :], group_prob[:, None, :], 0.0), axis=2))
    lifted = jnp.exp(expert_scores)
    return picked * lifted / lax.optimization_barrier(jnp.sum(lifted, axis=1, keepdims=True))

def reference(pool_input, pool_gate, pool_mix, pool_scale, out_proj, residual, norm_gain, routes, group_logits, expert_scores, w_gate, w_up, w_down):
    source = pool_input.astype(jnp.float32)
    extended = jnp.concatenate([jnp.zeros((POOL_WIDTH, reach_back), jnp.float32), source], axis=1)
    pooled = window_terms(extended, 0, 0, POOL_GROUP).astype(jnp.bfloat16)
    scales = POOL_WIDTH // POOL_GROUP
    grouped = pooled.reshape(scales, POOL_GROUP, TOKENS)
    mixed_rows = jnp.einsum('gct,gcd->tgd', grouped.astype(jnp.float32), pool_mix.astype(jnp.float32)).reshape(TOKENS, POOL_WIDTH)
    gating = jax.nn.sigmoid(pool_gate.astype(jnp.float32).T)
    branch = (gating * mixed_rows * pool_scale[None, :]).astype(jnp.bfloat16)
    hidden_state = (residual.astype(jnp.float32) + jnp.dot(branch, out_proj, preferred_element_type=jnp.float32)).astype(jnp.bfloat16)
    state_float = hidden_state.astype(jnp.float32)
    mean_square = lax.optimization_barrier(jnp.mean(state_float * state_float, axis=1, keepdims=True))
    normed = (state_float * lax.rsqrt(mean_square + epsilon) * norm_gain[None, :]).astype(jnp.bfloat16)
    weights = route_weights(routes, group_logits, expert_scores, EXPERTS // N_GROUPS)
    destination = jax.vmap(lambda row_block: slot_table(row_block, EXPERTS, CAP))(routes.reshape(N_SP, TOK_DEV, TOP))
    expert_of = destination // CAP
    rank_in = destination % CAP
    source_index = jnp.arange(N_SP, dtype=jnp.int32)[:, None]
    table_index = (expert_of * (N_SP * CAP) + source_index * CAP + rank_in).reshape(-1)
    token_index = jnp.arange(TOKENS * TOP, dtype=jnp.int32) // TOP
    sources = jnp.full((EXPERTS * N_SP * CAP,), TOKENS, jnp.int32).at[table_index].set(token_index)
    factors = jnp.zeros((EXPERTS * N_SP * CAP,), jnp.float32).at[table_index].set(weights.reshape(-1))
    padded = jnp.concatenate([normed, jnp.zeros((1, D), jnp.bfloat16)], axis=0)

    def expert_step(accumulated, inputs):
        sources_here, factors_here, gate_matrix, up_matrix, down_matrix = inputs
        picked_rows = padded[sources_here]
        gate_term = jnp.dot(picked_rows, gate_matrix, preferred_element_type=jnp.float32)
        up_term = jnp.dot(picked_rows, up_matrix, preferred_element_type=jnp.float32)
        activated = (jax.nn.silu(gate_term) * up_term).astype(jnp.bfloat16)
        result = jnp.dot(activated, down_matrix, preferred_element_type=jnp.float32).astype(jnp.bfloat16)
        accumulated = accumulated.at[sources_here].add(factors_here[:, None] * result.astype(jnp.float32))
        return (accumulated, None)
    accumulated, _ = lax.scan(expert_step, jnp.zeros((TOKENS + 1, D), jnp.float32), (sources.reshape(EXPERTS, N_SP * CAP), factors.reshape(EXPERTS, N_SP * CAP), w_gate, w_up, w_down))
    return (state_float + accumulated[:TOKENS]).astype(jnp.bfloat16)
```

```python
import jax
import jax.numpy as jnp
from jax import lax
from jax.experimental import pallas as pl
from jax.experimental.pallas import tpu as pltpu
from jax.sharding import Mesh, PartitionSpec as P

SPAN = 128
ROW_TILE = 144
GAIN_ROWS = 16
epsilon = 1e-06

TP = ("tg", "tl")


def pool_kernel(where_ref, edge_ref, own_ref, out_ref):
    scale, first = where_ref[0], where_ref[1]
    length = own_ref.shape[1]
    own = own_ref[...].astype(jnp.float32)
    layered = jnp.concatenate([edge_ref[...].astype(jnp.float32), own], axis=1)
    chosen = None
    stride = 1
    for octave in range(4):
        layered = layered + pltpu.roll(layered, stride, 1)
        stride *= 2
        chosen = layered if chosen is None else jnp.where(scale >= octave, layered, chosen)
    window = jnp.left_shift(2, scale)
    position = first + 1 + lax.broadcasted_iota(jnp.int32, own.shape, 1)
    counted = jnp.minimum(position, window).astype(jnp.float32)
    pooled = chosen[:, SPAN : SPAN + length] / counted - own
    out_ref[...] = pooled.astype(out_ref.dtype)


def pool(edge, own, scale, first):
    return pl.pallas_call(
        pool_kernel,
        out_shape=jax.ShapeDtypeStruct(own.shape, jnp.bfloat16),
        in_specs=[
            pl.BlockSpec(memory_space=pltpu.SMEM),
            pl.BlockSpec(memory_space=pltpu.VMEM),
            pl.BlockSpec(memory_space=pltpu.VMEM),
        ],
        name="pool",
    )(jnp.stack([scale, first]), edge, own)


def hidden_kernel(x_ref, extra_ref, gate_ref, up_ref, out_ref):
    parts, rows, width = x_ref.shape
    squares = jnp.zeros((rows, width), jnp.float32)
    scaled = []
    for part in range(parts):
        state = x_ref[part].astype(jnp.float32)
        squares += state * state
        extra = extra_ref[part].astype(jnp.float32)
        gain = extra[0:1] + extra[1:2] + extra[2:3]
        scaled.append((state * gain).astype(jnp.bfloat16))
    rows_in = jnp.concatenate(scaled, axis=1)
    mean = jnp.sum(squares, axis=1, keepdims=True) / (parts * width)
    factor = lax.rsqrt(mean + epsilon)
    gate = jnp.dot(rows_in, gate_ref[0], preferred_element_type=jnp.float32) * factor
    up = jnp.dot(rows_in, up_ref[0], preferred_element_type=jnp.float32) * factor
    out_ref[...] = (jax.nn.silu(gate) * up).astype(out_ref.dtype)


def hidden(everyone, w_gate, w_up, rows):
    parts, _, width = everyone.shape
    units = w_gate.shape[2]
    weight = pl.BlockSpec((1, parts * width, units), lambda i: (0, 0, 0))
    return pl.pallas_call(
        hidden_kernel,
        out_shape=jax.ShapeDtypeStruct((rows, units), jnp.bfloat16),
        grid=(rows // ROW_TILE,),
        in_specs=[
            pl.BlockSpec((parts, ROW_TILE, width), lambda i: (0, i, 0)),
            pl.BlockSpec((parts, GAIN_ROWS, width), lambda i: (0, rows // GAIN_ROWS, 0)),
            weight,
            weight,
        ],
        out_specs=pl.BlockSpec((ROW_TILE, units), lambda i: (i, 0)),
        name="hidden",
    )(everyone, everyone, w_gate, w_up)


def down_kernel(x_ref, down_ref, out_ref):
    rows_in = jnp.concatenate([x_ref[part] for part in range(x_ref.shape[0])], axis=1)
    result = jnp.dot(rows_in, down_ref[0], preferred_element_type=jnp.float32)
    out_ref[...] = result.astype(out_ref.dtype)


def down(everyone, w_down):
    parts, rows, units = everyone.shape
    width = w_down.shape[2]
    return pl.pallas_call(
        down_kernel,
        out_shape=jax.ShapeDtypeStruct((rows, width), jnp.bfloat16),
        grid=(rows // ROW_TILE,),
        in_specs=[
            pl.BlockSpec((parts, ROW_TILE, units), lambda i: (0, i, 0)),
            pl.BlockSpec((1, parts * units, width), lambda i: (0, 0, 0)),
        ],
        out_specs=pl.BlockSpec((ROW_TILE, width), lambda i: (i, 0)),
        name="down",
    )(everyone, w_down)


def combine_kernel(state_ref, slot_ref, weight_ref, returned_ref, out_ref):
    length, slots = state_ref.shape[0], returned_ref.shape[0]
    place = lax.broadcasted_iota(jnp.int32, (length, slots), 1)
    total = jnp.zeros(out_ref.shape, jnp.float32)
    for choice in range(slot_ref.shape[1]):
        pick = jnp.where(place == slot_ref[:, choice : choice + 1], 1.0, 0.0).astype(jnp.bfloat16)
        picked = jnp.dot(pick, returned_ref[...], preferred_element_type=jnp.float32)
        total += weight_ref[:, choice : choice + 1] * picked
    out_ref[...] = (state_ref[...].astype(jnp.float32) + total).astype(out_ref.dtype)


def combine(state, slots, weights, returned):
    return pl.pallas_call(
        combine_kernel,
        out_shape=jax.ShapeDtypeStruct(state.shape, jnp.bfloat16),
        name="combine",
    )(state, slots, weights, returned)


def slot_table(routes, experts, capacity):
    flattened = routes.reshape(-1)
    count = flattened.shape[0]
    onehot = (flattened[:, None] == jnp.arange(experts, dtype=jnp.int32)[None, :]).astype(jnp.bfloat16)
    row = lax.broadcasted_iota(jnp.int32, (count, count), 0)
    column = lax.broadcasted_iota(jnp.int32, (count, count), 1)
    earlier = (column < row).astype(jnp.bfloat16)
    before = jnp.dot(earlier, onehot, preferred_element_type=jnp.float32)
    ranked = jnp.sum(before * onehot.astype(jnp.float32), axis=1).astype(jnp.int32)
    return (flattened * capacity + ranked).reshape(routes.shape)


def route_weights(routes, group_logits, expert_scores, per_group):
    raised = jnp.exp(group_logits)
    group_prob = raised / jnp.sum(raised, axis=1, keepdims=True)
    owning_group = routes // per_group
    groups_iota = jnp.arange(group_logits.shape[1], dtype=jnp.int32)
    picked = jnp.sum(
        jnp.where(owning_group[:, :, None] == groups_iota[None, None, :], group_prob[:, None, :], 0.0),
        axis=2,
    )
    lifted = jnp.exp(expert_scores)
    return picked * lifted / jnp.sum(lifted, axis=1, keepdims=True)


def gain_rows(gain):
    rows, rest = [], gain
    for _ in range(3):
        head = lax.reduce_precision(rest, 8, 7)
        rows.append(head)
        rest = rest - head
    rows += [jnp.zeros_like(gain)] * (GAIN_ROWS - len(rows))
    return jnp.stack(rows).astype(jnp.bfloat16)


def per_device(
    pool_input,
    pool_gate,
    pool_mix,
    pool_scale,
    out_proj,
    residual,
    norm_gain,
    routes,
    group_logits,
    expert_scores,
    w_gate,
    w_up,
    w_down,
):
    channels, length = pool_input.shape
    blocks = lax.axis_size("sp")
    scale, quarter = lax.axis_index("tg"), lax.axis_index("tl")
    own_first = (scale * lax.axis_size("tl") + quarter) * channels
    edge = lax.ppermute(
        pool_input[:, length - SPAN :], "sp", [(i, i + 1) for i in range(blocks - 1)]
    )
    pooled = pool(edge, pool_input, scale, lax.axis_index("sp") * length)
    group = lax.all_gather(pooled, "tl", axis=0, tiled=True)
    mix = lax.dynamic_slice(
        pool_mix, (scale, 0, quarter * channels), (1, pool_mix.shape[1], channels)
    )[0]
    mixed = lax.dot_general(mix, group, (((0,), (0,)), ((), ())), preferred_element_type=jnp.float32)
    own_scale = lax.dynamic_slice(pool_scale, (own_first,), (channels,))
    branch = (jax.nn.sigmoid(pool_gate.astype(jnp.float32)) * mixed * own_scale[:, None]).astype(jnp.bfloat16)
    branches = lax.all_gather(branch, TP, axis=0, tiled=True)
    product = lax.dot_general(
        branches, out_proj, (((0,), (0,)), ((), ())), preferred_element_type=jnp.float32
    )
    state = (residual.astype(jnp.float32) + product).astype(jnp.bfloat16)

    experts = blocks * w_gate.shape[0]
    capacity = 3 * routes.shape[1] * length // (2 * experts)
    slots = slot_table(routes, experts, capacity)
    rows = experts * capacity
    place = jnp.arange(rows, dtype=jnp.int32)[:, None]
    spread = sum((place == slots[:, k][None, :]).astype(jnp.bfloat16) for k in range(slots.shape[1]))
    sent = jnp.dot(spread, state, preferred_element_type=jnp.float32).astype(jnp.bfloat16)
    arrived = lax.all_to_all(
        sent.reshape(blocks, capacity, -1), "sp", split_axis=0, concat_axis=0, tiled=True
    ).reshape(rows, -1)
    carried = jnp.concatenate([arrived, gain_rows(norm_gain)], axis=0)
    everyone = lax.all_gather(carried, TP, axis=0, tiled=False)
    activated = hidden(everyone, w_gate, w_up, rows)
    weights = route_weights(routes, group_logits, expert_scores, experts // group_logits.shape[1])
    units = lax.all_gather(activated, TP, axis=0, tiled=False)
    result = down(units, w_down)
    returned = lax.all_to_all(
        result.reshape(blocks, capacity, -1), "sp", split_axis=0, concat_axis=0, tiled=True
    ).reshape(rows, -1)
    return combine(state, slots, weights, returned)


def solution(mesh):
    fine = Mesh(mesh.devices.reshape(mesh.devices.shape[0], 4, -1), ("sp", *TP))
    placed = (
        P(TP, "sp"),
        P(TP, "sp"),
        P(),
        P(),
        P(None, TP),
        P("sp", TP),
        P(TP),
        P("sp", None),
        P("sp", None),
        P("sp", None),
        P("sp", None, TP),
        P("sp", None, TP),
        P("sp", None, TP),
    )
    return jax.shard_map(
        per_device, mesh=fine, in_specs=placed, out_specs=P("sp", TP), check_vma=False
    )
```

```python
import jax
import jax.numpy as jnp
from jax import lax
from jax.experimental import pallas as pl
from jax.experimental.pallas import tpu as pltpu
from jax.sharding import Mesh, PartitionSpec as P

SPAN = 128
GAIN_ROWS = 16
TOGETHER = 2
epsilon = 1e-06

X_PIECES = (1152,)
U_PIECES = (1152,)

TP = ("tg", "tl")


def vmem(mib):
    return pltpu.CompilerParams(vmem_limit_bytes=mib << 20)


def padded(rows):
    return -(-rows // 8) * 8


def pool_kernel(edge_ref, own_ref, out_ref):
    length = own_ref.shape[1]
    scale = lax.axis_index("tg")
    first = lax.axis_index("sp") * length
    own = own_ref[...].astype(jnp.float32)
    layered = jnp.concatenate([edge_ref[...].astype(jnp.float32), own], axis=1)
    chosen = None
    stride = 1
    for octave in range(4):
        layered = layered + pltpu.roll(layered, stride, 1)
        stride *= 2
        chosen = layered if chosen is None else jnp.where(scale >= octave, layered, chosen)
    window = jnp.left_shift(2, scale)
    position = first + 1 + lax.broadcasted_iota(jnp.int32, own.shape, 1)
    counted = jnp.minimum(position, window).astype(jnp.float32)
    pooled = chosen[:, SPAN : SPAN + length] / counted - own
    out_ref[...] = pooled.astype(out_ref.dtype)


def pool(edge, own):
    return pl.pallas_call(
        pool_kernel,
        out_shape=jax.ShapeDtypeStruct(own.shape, jnp.bfloat16),
        compiler_params=vmem(4),
        name="pool",
    )(edge, own)


def slot_kernel(experts, pitch, routes_ref, out_ref):
    choices, length = routes_ref.shape
    number = lax.broadcasted_iota(jnp.int32, (experts, length), 0)
    named = [(number == routes_ref[k : k + 1, :]).astype(jnp.float32) for k in range(choices)]
    earlier = lax.broadcasted_iota(jnp.int32, (length, length), 0) < lax.broadcasted_iota(
        jnp.int32, (length, length), 1
    )
    before = jnp.dot(
        sum(named).astype(jnp.bfloat16),
        jnp.where(earlier, 1.0, 0.0).astype(jnp.bfloat16),
        preferred_element_type=jnp.float32,
    )
    for k in range(choices):
        rank = jnp.sum(before * named[k], axis=0, keepdims=True).astype(jnp.int32)
        out_ref[k : k + 1, :] = routes_ref[k : k + 1, :] * pitch + rank


def slot_table(routes, experts, pitch):
    def kernel(routes_ref, out_ref):
        slot_kernel(experts, pitch, routes_ref, out_ref)

    return pl.pallas_call(
        kernel,
        out_shape=jax.ShapeDtypeStruct(routes.shape, jnp.int32),
        compiler_params=vmem(8),
        name="slots",
    )(routes)


def dispatch_kernel(state_ref, slot_ref, out_ref):
    blocks, capacity, _ = out_ref.shape
    pitch = padded(capacity)
    place = lax.broadcasted_iota(jnp.int32, (blocks * pitch, state_ref.shape[0]), 0)
    chosen = place == slot_ref[0:1, :]
    for k in range(1, slot_ref.shape[0]):
        chosen = chosen | (place == slot_ref[k : k + 1, :])
    spread = jnp.where(chosen, 1.0, 0.0).astype(jnp.bfloat16)
    rows = jnp.dot(spread, state_ref[...], preferred_element_type=jnp.float32)
    for block in range(blocks):
        out_ref[block] = rows[block * pitch : block * pitch + capacity].astype(out_ref.dtype)


def dispatch(state, slots, blocks, capacity):
    return pl.pallas_call(
        dispatch_kernel,
        out_shape=jax.ShapeDtypeStruct((blocks, capacity, state.shape[1]), jnp.bfloat16),
        compiler_params=vmem(12),
        name="dispatch",
    )(state, slots)


def compact_kernel(arrived_ref, gain_ref, *refs):
    outs, rows_ref = refs[:-1], refs[-1]
    blocks, capacity, _ = arrived_ref.shape
    for block in range(blocks):
        rows_ref[block * capacity : (block + 1) * capacity] = arrived_ref[block].astype(jnp.float32)
    start = 0
    for out_ref, count in zip(outs, X_PIECES):
        out_ref[0:count] = rows_ref[start : start + count].astype(jnp.bfloat16)
        start += count
    outs[-1][count : count + GAIN_ROWS] = gain_ref[...]


def compact(arrived, gains):
    rows, width = arrived.shape[0] * arrived.shape[1], arrived.shape[2]
    counts = (*X_PIECES[:-1], X_PIECES[-1] + GAIN_ROWS)
    return pl.pallas_call(
        compact_kernel,
        out_shape=[jax.ShapeDtypeStruct((count, width), jnp.bfloat16) for count in counts],
        scratch_shapes=[pltpu.VMEM((rows, width), jnp.float32)],
        compiler_params=vmem(8),
        name="compact",
    )(arrived, gains)


def hidden_kernel(*refs):
    pieces, count = len(X_PIECES), len(U_PIECES)
    x_refs, (extra_ref, gate_ref, up_ref) = refs[:pieces], refs[pieces : pieces + 3]
    outs = refs[pieces + 3 : pieces + 3 + count]
    squares_ref, gate_sum, up_sum = refs[pieces + 3 + count :]
    step, steps = pl.program_id(0), pl.num_programs(0)
    width = squares_ref.shape[1]

    @pl.when(step == 0)
    def _():
        squares_ref[...] = jnp.zeros_like(squares_ref)
        gate_sum[...] = jnp.zeros_like(gate_sum)
        up_sum[...] = jnp.zeros_like(up_sum)

    gains = []
    for part in range(TOGETHER):
        extra = extra_ref[part].astype(jnp.float32)
        gains.append(extra[0:1] + extra[1:2] + extra[2:3])
    start = 0
    for x_ref in x_refs:
        here = pl.ds(start, x_ref.shape[1])
        start += x_ref.shape[1]
        squares, scaled = squares_ref[here, :], []
        for part in range(TOGETHER):
            state = x_ref[part].astype(jnp.float32)
            squares += state * state
            scaled.append((state * gains[part]).astype(jnp.bfloat16))
        squares_ref[here, :] = squares
        rows_in = jnp.concatenate(scaled, axis=1)
        gate_sum[here, :] += jnp.dot(rows_in, gate_ref[0], preferred_element_type=jnp.float32)
        up_sum[here, :] += jnp.dot(rows_in, up_ref[0], preferred_element_type=jnp.float32)

    @pl.when(step == steps - 1)
    def _():
        begin = 0
        for out_ref in outs:
            there = pl.ds(begin, out_ref.shape[0])
            begin += out_ref.shape[0]
            mean = jnp.sum(squares_ref[there, :], axis=1, keepdims=True) / (steps * TOGETHER * width)
            factor = lax.rsqrt(mean + epsilon)
            gate, up = gate_sum[there, :] * factor, up_sum[there, :] * factor
            out_ref[...] = (jax.nn.silu(gate) * up).astype(out_ref.dtype)


def hidden(everyone, w_gate, w_up):
    parts, _, width = everyone[-1].shape
    rows, units = sum(X_PIECES), w_gate.shape[2]
    weight = pl.BlockSpec((1, TOGETHER * width, units), lambda i: (0, i, 0))
    last = X_PIECES[-1] // GAIN_ROWS
    return pl.pallas_call(
        hidden_kernel,
        out_shape=[jax.ShapeDtypeStruct((count, units), jnp.bfloat16) for count in U_PIECES],
        grid=(parts // TOGETHER,),
        in_specs=[
            *[pl.BlockSpec((TOGETHER, count, width), lambda i: (i, 0, 0)) for count in X_PIECES],
            pl.BlockSpec((TOGETHER, GAIN_ROWS, width), lambda i: (i, last, 0)),
            weight,
            weight,
        ],
        out_specs=[pl.BlockSpec((count, units), lambda i: (0, 0)) for count in U_PIECES],
        scratch_shapes=[
            pltpu.VMEM((rows, width), jnp.float32),
            pltpu.VMEM((rows, units), jnp.float32),
            pltpu.VMEM((rows, units), jnp.float32),
        ],
        name="hidden",
    )(*everyone, everyone[-1], w_gate, w_up)


def down_kernel(*refs):
    pieces = len(U_PIECES)
    u_refs, (down_ref, out_ref, total_ref) = refs[:pieces], refs[pieces:]
    step, steps = pl.program_id(0), pl.num_programs(0)

    @pl.when(step == 0)
    def _():
        total_ref[...] = jnp.zeros_like(total_ref)

    start = 0
    for u_ref in u_refs:
        here = pl.ds(start, u_ref.shape[1])
        start += u_ref.shape[1]
        rows_in = jnp.concatenate([u_ref[part] for part in range(TOGETHER)], axis=1)
        total_ref[here, :] += jnp.dot(rows_in, down_ref[0], preferred_element_type=jnp.float32)

    @pl.when(step == steps - 1)
    def _():
        blocks, capacity, _ = out_ref.shape
        for block in range(blocks):
            out_ref[block] = total_ref[block * capacity : (block + 1) * capacity].astype(out_ref.dtype)


def down(everyone, w_down, blocks, capacity):
    parts, _, units = everyone[-1].shape
    width = w_down.shape[2]
    return pl.pallas_call(
        down_kernel,
        out_shape=jax.ShapeDtypeStruct((blocks, capacity, width), jnp.bfloat16),
        grid=(parts // TOGETHER,),
        in_specs=[
            *[pl.BlockSpec((TOGETHER, count, units), lambda i: (i, 0, 0)) for count in U_PIECES],
            pl.BlockSpec((1, TOGETHER * units, width), lambda i: (0, i, 0)),
        ],
        out_specs=pl.BlockSpec((blocks, capacity, width), lambda i: (0, 0, 0)),
        scratch_shapes=[pltpu.VMEM((blocks * capacity, width), jnp.float32)],
        name="down",
    )(*everyone, w_down)


def combine_kernel(state_ref, slot_ref, weight_ref, returned_ref, out_ref, rows_ref):
    blocks, capacity, _ = returned_ref.shape
    pitch = padded(capacity)
    rows_ref[...] = jnp.zeros_like(rows_ref)
    for block in range(blocks):
        rows_ref[block * pitch : block * pitch + capacity] = returned_ref[block].astype(jnp.float32)
    rows = rows_ref[...].astype(jnp.bfloat16)
    place = lax.broadcasted_iota(jnp.int32, (state_ref.shape[0], blocks * pitch), 1)
    total = jnp.zeros(out_ref.shape, jnp.float32)
    for choice in range(slot_ref.shape[1]):
        pick = jnp.where(place == slot_ref[:, choice : choice + 1], 1.0, 0.0).astype(jnp.bfloat16)
        picked = jnp.dot(pick, rows, preferred_element_type=jnp.float32)
        total += weight_ref[:, choice : choice + 1] * picked
    out_ref[...] = (state_ref[...].astype(jnp.float32) + total).astype(out_ref.dtype)


def combine(state, slots, weights, returned):
    blocks, capacity, width = returned.shape
    return pl.pallas_call(
        combine_kernel,
        out_shape=jax.ShapeDtypeStruct(state.shape, jnp.bfloat16),
        scratch_shapes=[pltpu.VMEM((blocks * padded(capacity), width), jnp.float32)],
        compiler_params=vmem(12),
        name="combine",
    )(state, slots, weights, returned)


def route_weights(routes, group_logits, expert_scores, per_group):
    raised = jnp.exp(group_logits)
    group_prob = raised / jnp.sum(raised, axis=1, keepdims=True)
    owning_group = routes // per_group
    groups_iota = jnp.arange(group_logits.shape[1], dtype=jnp.int32)
    picked = jnp.sum(
        jnp.where(owning_group[:, :, None] == groups_iota[None, None, :], group_prob[:, None, :], 0.0),
        axis=2,
    )
    lifted = jnp.exp(expert_scores)
    return picked * lifted / jnp.sum(lifted, axis=1, keepdims=True)


def gain_rows(gain):
    row = lax.broadcasted_iota(jnp.int32, (GAIN_ROWS, gain.shape[0]), 0)
    rows, rest = jnp.zeros(row.shape, jnp.float32), gain[None, :]
    for k in range(3):
        head = lax.reduce_precision(rest, 8, 7)
        rows = jnp.where(row == k, head, rows)
        rest = rest - head
    return rows.astype(jnp.bfloat16)


def per_device(
    pool_input,
    pool_gate,
    pool_mix,
    pool_scale,
    out_proj,
    residual,
    norm_gain,
    routes,
    group_logits,
    expert_scores,
    w_gate,
    w_up,
    w_down,
):
    channels, length = pool_input.shape
    blocks = lax.axis_size("sp")
    experts = blocks * w_gate.shape[0]
    capacity = 3 * routes.shape[1] * length // (2 * experts)
    scale, quarter = lax.axis_index("tg"), lax.axis_index("tl")
    own_first = (scale * lax.axis_size("tl") + quarter) * channels
    edge = lax.ppermute(
        pool_input[:, length - SPAN :], "sp", [(i, i + 1) for i in range(blocks - 1)]
    )
    slots = slot_table(routes.T, experts, padded(capacity))
    gains = gain_rows(norm_gain)
    pooled = pool(edge, pool_input)
    group = lax.all_gather(pooled, "tl", axis=0, tiled=True)
    mix = lax.dynamic_slice(
        pool_mix, (scale, 0, quarter * channels), (1, pool_mix.shape[1], channels)
    )[0]
    mixed = lax.dot_general(mix, group, (((0,), (0,)), ((), ())), preferred_element_type=jnp.float32)
    own_scale = lax.dynamic_slice(pool_scale, (own_first,), (channels,))
    branch = (jax.nn.sigmoid(pool_gate.astype(jnp.float32)) * mixed * own_scale[:, None]).astype(jnp.bfloat16)
    branches = lax.all_gather(branch, TP, axis=0, tiled=True)
    product = lax.dot_general(
        branches, out_proj, (((0,), (0,)), ((), ())), preferred_element_type=jnp.float32
    )
    state = (residual.astype(jnp.float32) + product).astype(jnp.bfloat16)

    sent = dispatch(state, slots, blocks, capacity)
    arrived = lax.all_to_all(sent, "sp", split_axis=0, concat_axis=0, tiled=True)
    everyone = [lax.all_gather(piece, TP, axis=0, tiled=False) for piece in compact(arrived, gains)]
    activated = hidden(everyone, w_gate, w_up)
    units = [lax.all_gather(piece, TP, axis=0, tiled=False) for piece in activated]
    result = down(units, w_down, blocks, capacity)
    returned = lax.all_to_all(result, "sp", split_axis=0, concat_axis=0, tiled=True)
    weights = route_weights(routes, group_logits, expert_scores, experts // group_logits.shape[1])
    return combine(state, slots.T, weights, returned)


def solution(mesh):
    fine = Mesh(mesh.devices.reshape(mesh.devices.shape[0], 4, -1), ("sp", *TP))
    placed = (
        P(TP, "sp"),
        P(TP, "sp"),
        P(),
        P(),
        P(None, TP),
        P("sp", TP),
        P(TP),
        P("sp", None),
        P("sp", None),
        P("sp", None),
        P("sp", None, TP),
        P("sp", None, TP),
        P("sp", None, TP),
    )
    return jax.shard_map(
        per_device, mesh=fine, in_specs=placed, out_specs=P("sp", TP), check_vma=False
    )
```

```python
import jax
import jax.numpy as jnp
from jax import lax
from jax.experimental import pallas as pl
from jax.experimental.pallas import tpu as pltpu
from jax.sharding import Mesh, PartitionSpec as P

SPAN = 128
GAIN_ROWS = 16
TOGETHER = 2
epsilon = 1e-06

X_PIECES = (720, 208, 224)
U_PIECES = (864, 96, 96, 96)

TP = ("tg", "tl")


def vmem(mib):
    return pltpu.CompilerParams(vmem_limit_bytes=mib << 20)


def padded(rows):
    return -(-rows // 8) * 8


def pool_kernel(edge_ref, own_ref, out_ref):
    length = own_ref.shape[1]
    scale = lax.axis_index("tg")
    first = lax.axis_index("sp") * length
    own = own_ref[...].astype(jnp.float32)
    layered = jnp.concatenate([edge_ref[...].astype(jnp.float32), own], axis=1)
    chosen = None
    stride = 1
    for octave in range(4):
        layered = layered + pltpu.roll(layered, stride, 1)
        stride *= 2
        chosen = layered if chosen is None else jnp.where(scale >= octave, layered, chosen)
    window = jnp.left_shift(2, scale)
    position = first + 1 + lax.broadcasted_iota(jnp.int32, own.shape, 1)
    counted = jnp.minimum(position, window).astype(jnp.float32)
    pooled = chosen[:, SPAN : SPAN + length] / counted - own
    out_ref[...] = pooled.astype(out_ref.dtype)


def pool(edge, own):
    return pl.pallas_call(
        pool_kernel,
        out_shape=jax.ShapeDtypeStruct(own.shape, jnp.bfloat16),
        compiler_params=vmem(4),
        name="pool",
    )(edge, own)


def slot_kernel(experts, pitch, routes_ref, out_ref):
    choices, length = routes_ref.shape
    number = lax.broadcasted_iota(jnp.int32, (experts, length), 0)
    named = [(number == routes_ref[k : k + 1, :]).astype(jnp.float32) for k in range(choices)]
    earlier = lax.broadcasted_iota(jnp.int32, (length, length), 0) < lax.broadcasted_iota(
        jnp.int32, (length, length), 1
    )
    before = jnp.dot(
        sum(named).astype(jnp.bfloat16),
        jnp.where(earlier, 1.0, 0.0).astype(jnp.bfloat16),
        preferred_element_type=jnp.float32,
    )
    for k in range(choices):
        rank = jnp.sum(before * named[k], axis=0, keepdims=True).astype(jnp.int32)
        out_ref[k : k + 1, :] = routes_ref[k : k + 1, :] * pitch + rank


def slot_table(routes, experts, pitch):
    def kernel(routes_ref, out_ref):
        slot_kernel(experts, pitch, routes_ref, out_ref)

    return pl.pallas_call(
        kernel,
        out_shape=jax.ShapeDtypeStruct(routes.shape, jnp.int32),
        compiler_params=vmem(8),
        name="slots",
    )(routes)


def dispatch_kernel(state_ref, slot_ref, out_ref):
    blocks, capacity, _ = out_ref.shape
    pitch = padded(capacity)
    place = lax.broadcasted_iota(jnp.int32, (blocks * pitch, state_ref.shape[0]), 0)
    chosen = place == slot_ref[0:1, :]
    for k in range(1, slot_ref.shape[0]):
        chosen = chosen | (place == slot_ref[k : k + 1, :])
    spread = jnp.where(chosen, 1.0, 0.0).astype(jnp.bfloat16)
    rows = jnp.dot(spread, state_ref[...], preferred_element_type=jnp.float32)
    for block in range(blocks):
        out_ref[block] = rows[block * pitch : block * pitch + capacity].astype(out_ref.dtype)


def dispatch(state, slots, blocks, capacity):
    return pl.pallas_call(
        dispatch_kernel,
        out_shape=jax.ShapeDtypeStruct((blocks, capacity, state.shape[1]), jnp.bfloat16),
        compiler_params=vmem(12),
        name="dispatch",
    )(state, slots)


def compact_kernel(arrived_ref, gain_ref, *refs):
    outs, rows_ref = refs[:-1], refs[-1]
    blocks, capacity, _ = arrived_ref.shape
    for block in range(blocks):
        rows_ref[block * capacity : (block + 1) * capacity] = arrived_ref[block].astype(jnp.float32)
    start = 0
    for out_ref, count in zip(outs, X_PIECES):
        out_ref[0:count] = rows_ref[start : start + count].astype(jnp.bfloat16)
        start += count
    outs[-1][count : count + GAIN_ROWS] = gain_ref[...]


def compact(arrived, gains):
    rows, width = arrived.shape[0] * arrived.shape[1], arrived.shape[2]
    counts = (*X_PIECES[:-1], X_PIECES[-1] + GAIN_ROWS)
    return pl.pallas_call(
        compact_kernel,
        out_shape=[jax.ShapeDtypeStruct((count, width), jnp.bfloat16) for count in counts],
        scratch_shapes=[pltpu.VMEM((rows, width), jnp.float32)],
        compiler_params=vmem(8),
        name="compact",
    )(arrived, gains)


def hidden_kernel(*refs):
    pieces, count = len(X_PIECES), len(U_PIECES)
    x_refs, (extra_ref, gate_ref, up_ref) = refs[:pieces], refs[pieces : pieces + 3]
    outs = refs[pieces + 3 : pieces + 3 + count]
    squares_ref, gate_sum, up_sum = refs[pieces + 3 + count :]
    step, steps = pl.program_id(0), pl.num_programs(0)
    width = squares_ref.shape[1]

    @pl.when(step == 0)
    def _():
        squares_ref[...] = jnp.zeros_like(squares_ref)
        gate_sum[...] = jnp.zeros_like(gate_sum)
        up_sum[...] = jnp.zeros_like(up_sum)

    gains = []
    for part in range(TOGETHER):
        extra = extra_ref[part].astype(jnp.float32)
        gains.append(extra[0:1] + extra[1:2] + extra[2:3])
    start = 0
    for x_ref in x_refs:
        here = pl.ds(start, x_ref.shape[1])
        start += x_ref.shape[1]
        squares, scaled = squares_ref[here, :], []
        for part in range(TOGETHER):
            state = x_ref[part].astype(jnp.float32)
            squares += state * state
            scaled.append((state * gains[part]).astype(jnp.bfloat16))
        squares_ref[here, :] = squares
        rows_in = jnp.concatenate(scaled, axis=1)
        gate_sum[here, :] += jnp.dot(rows_in, gate_ref[0], preferred_element_type=jnp.float32)
        up_sum[here, :] += jnp.dot(rows_in, up_ref[0], preferred_element_type=jnp.float32)

    @pl.when(step == steps - 1)
    def _():
        begin = 0
        for out_ref in outs:
            there = pl.ds(begin, out_ref.shape[0])
            begin += out_ref.shape[0]
            mean = jnp.sum(squares_ref[there, :], axis=1, keepdims=True) / (steps * TOGETHER * width)
            factor = lax.rsqrt(mean + epsilon)
            gate, up = gate_sum[there, :] * factor, up_sum[there, :] * factor
            out_ref[...] = (jax.nn.silu(gate) * up).astype(out_ref.dtype)


def hidden(everyone, w_gate, w_up):
    parts, _, width = everyone[-1].shape
    rows, units = sum(X_PIECES), w_gate.shape[2]
    weight = pl.BlockSpec((1, TOGETHER * width, units), lambda i: (0, i, 0))
    last = X_PIECES[-1] // GAIN_ROWS
    return pl.pallas_call(
        hidden_kernel,
        out_shape=[jax.ShapeDtypeStruct((count, units), jnp.bfloat16) for count in U_PIECES],
        grid=(parts // TOGETHER,),
        in_specs=[
            *[pl.BlockSpec((TOGETHER, count, width), lambda i: (i, 0, 0)) for count in X_PIECES],
            pl.BlockSpec((TOGETHER, GAIN_ROWS, width), lambda i: (i, last, 0)),
            weight,
            weight,
        ],
        out_specs=[pl.BlockSpec((count, units), lambda i: (0, 0)) for count in U_PIECES],
        scratch_shapes=[
            pltpu.VMEM((rows, width), jnp.float32),
            pltpu.VMEM((rows, units), jnp.float32),
            pltpu.VMEM((rows, units), jnp.float32),
        ],
        name="hidden",
    )(*everyone, everyone[-1], w_gate, w_up)


def down_kernel(*refs):
    pieces = len(U_PIECES)
    u_refs, (down_ref, out_ref, total_ref) = refs[:pieces], refs[pieces:]
    step, steps = pl.program_id(0), pl.num_programs(0)

    @pl.when(step == 0)
    def _():
        total_ref[...] = jnp.zeros_like(total_ref)

    start = 0
    for u_ref in u_refs:
        here = pl.ds(start, u_ref.shape[1])
        start += u_ref.shape[1]
        rows_in = jnp.concatenate([u_ref[part] for part in range(TOGETHER)], axis=1)
        total_ref[here, :] += jnp.dot(rows_in, down_ref[0], preferred_element_type=jnp.float32)

    @pl.when(step == steps - 1)
    def _():
        blocks, capacity, _ = out_ref.shape
        for block in range(blocks):
            out_ref[block] = total_ref[block * capacity : (block + 1) * capacity].astype(out_ref.dtype)


def down(everyone, w_down, blocks, capacity):
    parts, _, units = everyone[-1].shape
    width = w_down.shape[2]
    return pl.pallas_call(
        down_kernel,
        out_shape=jax.ShapeDtypeStruct((blocks, capacity, width), jnp.bfloat16),
        grid=(parts // TOGETHER,),
        in_specs=[
            *[pl.BlockSpec((TOGETHER, count, units), lambda i: (i, 0, 0)) for count in U_PIECES],
            pl.BlockSpec((1, TOGETHER * units, width), lambda i: (0, i, 0)),
        ],
        out_specs=pl.BlockSpec((blocks, capacity, width), lambda i: (0, 0, 0)),
        scratch_shapes=[pltpu.VMEM((blocks * capacity, width), jnp.float32)],
        name="down",
    )(*everyone, w_down)


def combine_kernel(state_ref, slot_ref, weight_ref, returned_ref, out_ref, rows_ref):
    blocks, capacity, _ = returned_ref.shape
    pitch = padded(capacity)
    rows_ref[...] = jnp.zeros_like(rows_ref)
    for block in range(blocks):
        rows_ref[block * pitch : block * pitch + capacity] = returned_ref[block].astype(jnp.float32)
    rows = rows_ref[...].astype(jnp.bfloat16)
    place = lax.broadcasted_iota(jnp.int32, (state_ref.shape[0], blocks * pitch), 1)
    total = jnp.zeros(out_ref.shape, jnp.float32)
    for choice in range(slot_ref.shape[1]):
        pick = jnp.where(place == slot_ref[:, choice : choice + 1], 1.0, 0.0).astype(jnp.bfloat16)
        picked = jnp.dot(pick, rows, preferred_element_type=jnp.float32)
        total += weight_ref[:, choice : choice + 1] * picked
    out_ref[...] = (state_ref[...].astype(jnp.float32) + total).astype(out_ref.dtype)


def combine(state, slots, weights, returned):
    blocks, capacity, width = returned.shape
    return pl.pallas_call(
        combine_kernel,
        out_shape=jax.ShapeDtypeStruct(state.shape, jnp.bfloat16),
        scratch_shapes=[pltpu.VMEM((blocks * padded(capacity), width), jnp.float32)],
        compiler_params=vmem(12),
        name="combine",
    )(state, slots, weights, returned)


def route_weights(routes, group_logits, expert_scores, per_group):
    raised = jnp.exp(group_logits)
    group_prob = raised / jnp.sum(raised, axis=1, keepdims=True)
    owning_group = routes // per_group
    groups_iota = jnp.arange(group_logits.shape[1], dtype=jnp.int32)
    picked = jnp.sum(
        jnp.where(owning_group[:, :, None] == groups_iota[None, None, :], group_prob[:, None, :], 0.0),
        axis=2,
    )
    lifted = jnp.exp(expert_scores)
    return picked * lifted / jnp.sum(lifted, axis=1, keepdims=True)


def gain_rows(gain):
    row = lax.broadcasted_iota(jnp.int32, (GAIN_ROWS, gain.shape[0]), 0)
    rows, rest = jnp.zeros(row.shape, jnp.float32), gain[None, :]
    for k in range(3):
        head = lax.reduce_precision(rest, 8, 7)
        rows = jnp.where(row == k, head, rows)
        rest = rest - head
    return rows.astype(jnp.bfloat16)


def per_device(
    pool_input,
    pool_gate,
    pool_mix,
    pool_scale,
    out_proj,
    residual,
    norm_gain,
    routes,
    group_logits,
    expert_scores,
    w_gate,
    w_up,
    w_down,
):
    channels, length = pool_input.shape
    blocks = lax.axis_size("sp")
    experts = blocks * w_gate.shape[0]
    capacity = 3 * routes.shape[1] * length // (2 * experts)
    scale, quarter = lax.axis_index("tg"), lax.axis_index("tl")
    own_first = (scale * lax.axis_size("tl") + quarter) * channels
    edge = lax.ppermute(
        pool_input[:, length - SPAN :], "sp", [(i, i + 1) for i in range(blocks - 1)]
    )
    slots = slot_table(routes.T, experts, padded(capacity))
    gains = gain_rows(norm_gain)
    pooled = pool(edge, pool_input)
    group = lax.all_gather(pooled, "tl", axis=0, tiled=True)
    mix = lax.dynamic_slice(
        pool_mix, (scale, 0, quarter * channels), (1, pool_mix.shape[1], channels)
    )[0]
    mixed = lax.dot_general(mix, group, (((0,), (0,)), ((), ())), preferred_element_type=jnp.float32)
    own_scale = lax.dynamic_slice(pool_scale, (own_first,), (channels,))
    branch = (jax.nn.sigmoid(pool_gate.astype(jnp.float32)) * mixed * own_scale[:, None]).astype(jnp.bfloat16)
    branches = lax.all_gather(branch, TP, axis=0, tiled=True)
    product = lax.dot_general(
        branches, out_proj, (((0,), (0,)), ((), ())), preferred_element_type=jnp.float32
    )
    state = (residual.astype(jnp.float32) + product).astype(jnp.bfloat16)

    sent = dispatch(state, slots, blocks, capacity)
    arrived = lax.all_to_all(sent, "sp", split_axis=0, concat_axis=0, tiled=True)
    everyone = [lax.all_gather(piece, TP, axis=0, tiled=False) for piece in compact(arrived, gains)]
    activated = hidden(everyone, w_gate, w_up)
    units = [lax.all_gather(piece, TP, axis=0, tiled=False) for piece in activated]
    result = down(units, w_down, blocks, capacity)
    returned = lax.all_to_all(result, "sp", split_axis=0, concat_axis=0, tiled=True)
    weights = route_weights(routes, group_logits, expert_scores, experts // group_logits.shape[1])
    return combine(state, slots.T, weights, returned)


def solution(mesh):
    fine = Mesh(mesh.devices.reshape(mesh.devices.shape[0], 4, -1), ("sp", *TP))
    placed = (
        P(TP, "sp"),
        P(TP, "sp"),
        P(),
        P(),
        P(None, TP),
        P("sp", TP),
        P(TP),
        P("sp", None),
        P("sp", None),
        P("sp", None),
        P("sp", None, TP),
        P("sp", None, TP),
        P("sp", None, TP),
    )
    return jax.shard_map(
        per_device, mesh=fine, in_specs=placed, out_specs=P("sp", TP), check_vma=False
    )
```

```python
import jax
import jax.numpy as jnp
from jax import lax
from jax.experimental import pallas as pl
from jax.experimental.pallas import tpu as pltpu
from jax.sharding import Mesh, PartitionSpec as P

SPAN = 128
GAIN_ROWS = 16
TOGETHER = 4
DOWN_TOGETHER = 2
epsilon = 1e-06

X_PIECES = (1152,)
U_PIECES = (928, 112, 112)

TP = ("tg", "tl")


def vmem(mib):
    return pltpu.CompilerParams(vmem_limit_bytes=mib << 20)


def padded(rows):
    return -(-rows // 8) * 8


def pool_kernel(edge_ref, own_ref, out_ref):
    length = own_ref.shape[1]
    scale = lax.axis_index("tg")
    first = lax.axis_index("sp") * length
    own = own_ref[...].astype(jnp.float32)
    layered = jnp.concatenate([edge_ref[...].astype(jnp.float32), own], axis=1)
    chosen = None
    stride = 1
    for octave in range(4):
        layered = layered + pltpu.roll(layered, stride, 1)
        stride *= 2
        chosen = layered if chosen is None else jnp.where(scale >= octave, layered, chosen)
    window = jnp.left_shift(2, scale)
    position = first + 1 + lax.broadcasted_iota(jnp.int32, own.shape, 1)
    counted = jnp.minimum(position, window).astype(jnp.float32)
    pooled = chosen[:, SPAN : SPAN + length] / counted - own
    out_ref[...] = pooled.astype(out_ref.dtype)


def pool(edge, own):
    return pl.pallas_call(
        pool_kernel,
        out_shape=jax.ShapeDtypeStruct(own.shape, jnp.bfloat16),
        compiler_params=vmem(4),
        name="pool",
    )(edge, own)


def slot_kernel(experts, pitch, routes_ref, out_ref):
    choices, length = routes_ref.shape
    number = lax.broadcasted_iota(jnp.int32, (experts, length), 0)
    named = [(number == routes_ref[k : k + 1, :]).astype(jnp.float32) for k in range(choices)]
    earlier = lax.broadcasted_iota(jnp.int32, (length, length), 0) < lax.broadcasted_iota(
        jnp.int32, (length, length), 1
    )
    before = jnp.dot(
        sum(named).astype(jnp.bfloat16),
        jnp.where(earlier, 1.0, 0.0).astype(jnp.bfloat16),
        preferred_element_type=jnp.float32,
    )
    for k in range(choices):
        rank = jnp.sum(before * named[k], axis=0, keepdims=True).astype(jnp.int32)
        out_ref[k : k + 1, :] = routes_ref[k : k + 1, :] * pitch + rank


def slot_table(routes, experts, pitch):
    def kernel(routes_ref, out_ref):
        slot_kernel(experts, pitch, routes_ref, out_ref)

    return pl.pallas_call(
        kernel,
        out_shape=jax.ShapeDtypeStruct(routes.shape, jnp.int32),
        compiler_params=vmem(8),
        name="slots",
    )(routes)


def dispatch_kernel(state_ref, slot_ref, out_ref):
    blocks, capacity, _ = out_ref.shape
    pitch = padded(capacity)
    place = lax.broadcasted_iota(jnp.int32, (blocks * pitch, state_ref.shape[0]), 0)
    chosen = place == slot_ref[0:1, :]
    for k in range(1, slot_ref.shape[0]):
        chosen = chosen | (place == slot_ref[k : k + 1, :])
    spread = jnp.where(chosen, 1.0, 0.0).astype(jnp.bfloat16)
    rows = jnp.dot(spread, state_ref[...], preferred_element_type=jnp.float32)
    for block in range(blocks):
        out_ref[block] = rows[block * pitch : block * pitch + capacity].astype(out_ref.dtype)


def dispatch(state, slots, blocks, capacity):
    return pl.pallas_call(
        dispatch_kernel,
        out_shape=jax.ShapeDtypeStruct((blocks, capacity, state.shape[1]), jnp.bfloat16),
        compiler_params=vmem(12),
        name="dispatch",
    )(state, slots)


def compact_kernel(arrived_ref, gain_ref, *refs):
    outs, rows_ref = refs[:-1], refs[-1]
    blocks, capacity, _ = arrived_ref.shape
    for block in range(blocks):
        rows_ref[block * capacity : (block + 1) * capacity] = arrived_ref[block].astype(jnp.float32)
    start = 0
    for out_ref, count in zip(outs, X_PIECES):
        out_ref[0:count] = rows_ref[start : start + count].astype(jnp.bfloat16)
        start += count
    outs[-1][count : count + GAIN_ROWS] = gain_ref[...]


def compact(arrived, gains):
    rows, width = arrived.shape[0] * arrived.shape[1], arrived.shape[2]
    counts = (*X_PIECES[:-1], X_PIECES[-1] + GAIN_ROWS)
    return pl.pallas_call(
        compact_kernel,
        out_shape=[jax.ShapeDtypeStruct((count, width), jnp.bfloat16) for count in counts],
        scratch_shapes=[pltpu.VMEM((rows, width), jnp.float32)],
        compiler_params=vmem(8),
        name="compact",
    )(arrived, gains)


def parts_of(hbm_refs, buffers, sems, part):
    return [
        pltpu.make_async_copy(hbm.at[part], buffer.at[part], sems.at[part, piece])
        for piece, (hbm, buffer) in enumerate(zip(hbm_refs, buffers))
    ]


def hidden_kernel(*refs):
    pieces, count = len(X_PIECES), len(U_PIECES)
    x_hbm, (gate_hbm, up_hbm) = refs[:pieces], refs[pieces : pieces + 2]
    outs, scratch = refs[pieces + 2 : pieces + 2 + count], refs[pieces + 2 + count :]
    x_refs, (gate_ref, up_ref, squares_ref, gate_sum, up_sum, x_sems, w_sems) = scratch[:pieces], scratch[pieces:]
    parts, width = x_refs[0].shape[0], x_refs[0].shape[2]
    depth = TOGETHER * width
    chunks = parts // TOGETHER

    def weights_of(chunk):
        here = pl.ds(chunk * depth, depth)
        return [
            pltpu.make_async_copy(hbm.at[0, here], ref.at[here], w_sems.at[chunk, k])
            for k, (hbm, ref) in enumerate(((gate_hbm, gate_ref), (up_hbm, up_ref)))
        ]

    copies = []
    for chunk in range(chunks):
        here = weights_of(chunk)
        for part in range(chunk * TOGETHER, (chunk + 1) * TOGETHER):
            here += parts_of(x_hbm, x_refs, x_sems, part)
        for copy in here:
            copy.start()
        copies.append(here)
    for chunk in range(chunks):
        for copy in copies[chunk]:
            copy.wait()
        mine = range(chunk * TOGETHER, (chunk + 1) * TOGETHER)
        gains = []
        for part in mine:
            extra = x_refs[-1][part, pl.ds(X_PIECES[-1], GAIN_ROWS), :].astype(jnp.float32)
            gains.append(extra[0:1] + extra[1:2] + extra[2:3])
        start = 0
        for x_ref, rows in zip(x_refs, X_PIECES):
            here = pl.ds(start, rows)
            start += rows
            squares, scaled = None, []
            for part, gain in zip(mine, gains):
                state = x_ref[part, pl.ds(0, rows), :].astype(jnp.float32)
                squares = state * state if squares is None else squares + state * state
                scaled.append((state * gain).astype(jnp.bfloat16))
            rows_in = jnp.concatenate(scaled, axis=1)
            deep = pl.ds(chunk * depth, depth)
            gate = jnp.dot(rows_in, gate_ref[deep, :], preferred_element_type=jnp.float32)
            up = jnp.dot(rows_in, up_ref[deep, :], preferred_element_type=jnp.float32)
            if chunk == 0:
                squares_ref[here, :], gate_sum[here, :], up_sum[here, :] = squares, gate, up
            else:
                squares_ref[here, :] += squares
                gate_sum[here, :] += gate
                up_sum[here, :] += up
    begin = 0
    for out_ref in outs:
        there = pl.ds(begin, out_ref.shape[0])
        begin += out_ref.shape[0]
        mean = jnp.sum(squares_ref[there, :], axis=1, keepdims=True) / (parts * width)
        factor = lax.rsqrt(mean + epsilon)
        gate, up = gate_sum[there, :] * factor, up_sum[there, :] * factor
        out_ref[...] = (jax.nn.silu(gate) * up).astype(out_ref.dtype)


def hidden(everyone, w_gate, w_up):
    parts, _, width = everyone[-1].shape
    rows, units = sum(X_PIECES), w_gate.shape[2]
    hbm = pl.BlockSpec(memory_space=pltpu.HBM)
    return pl.pallas_call(
        hidden_kernel,
        out_shape=[jax.ShapeDtypeStruct((count, units), jnp.bfloat16) for count in U_PIECES],
        in_specs=[hbm] * (len(everyone) + 2),
        scratch_shapes=[
            *[pltpu.VMEM(piece.shape, piece.dtype) for piece in everyone],
            pltpu.VMEM(w_gate.shape[1:], w_gate.dtype),
            pltpu.VMEM(w_up.shape[1:], w_up.dtype),
            pltpu.VMEM((rows, width), jnp.float32),
            pltpu.VMEM((rows, units), jnp.float32),
            pltpu.VMEM((rows, units), jnp.float32),
            pltpu.SemaphoreType.DMA((parts, len(everyone))),
            pltpu.SemaphoreType.DMA((parts // TOGETHER, 2)),
        ],
        name="hidden",
    )(*everyone, w_gate, w_up)


def down_kernel(*refs):
    pieces = len(U_PIECES)
    u_hbm, (down_hbm, out_ref), scratch = refs[:pieces], refs[pieces : pieces + 2], refs[pieces + 2 :]
    u_refs, (down_ref, total_ref, u_sems, w_sems) = scratch[:pieces], scratch[pieces:]
    parts, _, units = u_refs[0].shape
    depth = DOWN_TOGETHER * units
    chunks = parts // DOWN_TOGETHER
    copies = []
    for chunk in range(chunks):
        deep = pl.ds(chunk * depth, depth)
        here = [pltpu.make_async_copy(down_hbm.at[0, deep], down_ref.at[deep], w_sems.at[chunk])]
        for part in range(chunk * DOWN_TOGETHER, (chunk + 1) * DOWN_TOGETHER):
            here += parts_of(u_hbm, u_refs, u_sems, part)
        for copy in here:
            copy.start()
        copies.append(here)
    for chunk in range(chunks):
        for copy in copies[chunk]:
            copy.wait()
        start = 0
        for u_ref in u_refs:
            here = pl.ds(start, u_ref.shape[1])
            start += u_ref.shape[1]
            rows_in = jnp.concatenate(
                [u_ref[part] for part in range(chunk * DOWN_TOGETHER, (chunk + 1) * DOWN_TOGETHER)], axis=1
            )
            product = jnp.dot(
                rows_in, down_ref[pl.ds(chunk * depth, depth), :], preferred_element_type=jnp.float32
            )
            if chunk == 0:
                total_ref[here, :] = product
            else:
                total_ref[here, :] += product
    blocks, capacity, _ = out_ref.shape
    for block in range(blocks):
        out_ref[block] = total_ref[block * capacity : (block + 1) * capacity].astype(out_ref.dtype)


def down(everyone, w_down, blocks, capacity):
    parts = everyone[0].shape[0]
    width = w_down.shape[2]
    hbm = pl.BlockSpec(memory_space=pltpu.HBM)
    return pl.pallas_call(
        down_kernel,
        out_shape=jax.ShapeDtypeStruct((blocks, capacity, width), jnp.bfloat16),
        in_specs=[hbm] * (len(everyone) + 1),
        scratch_shapes=[
            *[pltpu.VMEM(piece.shape, piece.dtype) for piece in everyone],
            pltpu.VMEM(w_down.shape[1:], w_down.dtype),
            pltpu.VMEM((blocks * capacity, width), jnp.float32),
            pltpu.SemaphoreType.DMA((parts, len(everyone))),
            pltpu.SemaphoreType.DMA((parts // DOWN_TOGETHER,)),
        ],
        name="down",
    )(*everyone, w_down)


def combine_kernel(state_ref, slot_ref, weight_ref, returned_ref, out_ref, rows_ref):
    blocks, capacity, _ = returned_ref.shape
    pitch = padded(capacity)
    rows_ref[...] = jnp.zeros_like(rows_ref)
    for block in range(blocks):
        rows_ref[block * pitch : block * pitch + capacity] = returned_ref[block].astype(jnp.float32)
    rows = rows_ref[...].astype(jnp.bfloat16)
    place = lax.broadcasted_iota(jnp.int32, (state_ref.shape[0], blocks * pitch), 1)
    total = jnp.zeros(out_ref.shape, jnp.float32)
    for choice in range(slot_ref.shape[1]):
        pick = jnp.where(place == slot_ref[:, choice : choice + 1], 1.0, 0.0).astype(jnp.bfloat16)
        picked = jnp.dot(pick, rows, preferred_element_type=jnp.float32)
        total += weight_ref[:, choice : choice + 1] * picked
    out_ref[...] = (state_ref[...].astype(jnp.float32) + total).astype(out_ref.dtype)


def combine(state, slots, weights, returned):
    blocks, capacity, width = returned.shape
    return pl.pallas_call(
        combine_kernel,
        out_shape=jax.ShapeDtypeStruct(state.shape, jnp.bfloat16),
        scratch_shapes=[pltpu.VMEM((blocks * padded(capacity), width), jnp.float32)],
        compiler_params=vmem(12),
        name="combine",
    )(state, slots, weights, returned)


def route_weights(routes, group_logits, expert_scores, per_group):
    raised = jnp.exp(group_logits)
    group_prob = raised / jnp.sum(raised, axis=1, keepdims=True)
    owning_group = routes // per_group
    groups_iota = jnp.arange(group_logits.shape[1], dtype=jnp.int32)
    picked = jnp.sum(
        jnp.where(owning_group[:, :, None] == groups_iota[None, None, :], group_prob[:, None, :], 0.0),
        axis=2,
    )
    lifted = jnp.exp(expert_scores)
    return picked * lifted / jnp.sum(lifted, axis=1, keepdims=True)


def gain_rows(gain):
    row = lax.broadcasted_iota(jnp.int32, (GAIN_ROWS, gain.shape[0]), 0)
    rows, rest = jnp.zeros(row.shape, jnp.float32), gain[None, :]
    for k in range(3):
        head = lax.reduce_precision(rest, 8, 7)
        rows = jnp.where(row == k, head, rows)
        rest = rest - head
    return rows.astype(jnp.bfloat16)


def per_device(
    pool_input,
    pool_gate,
    pool_mix,
    pool_scale,
    out_proj,
    residual,
    norm_gain,
    routes,
    group_logits,
    expert_scores,
    w_gate,
    w_up,
    w_down,
):
    channels, length = pool_input.shape
    blocks = lax.axis_size("sp")
    experts = blocks * w_gate.shape[0]
    capacity = 3 * routes.shape[1] * length // (2 * experts)
    scale, quarter = lax.axis_index("tg"), lax.axis_index("tl")
    own_first = (scale * lax.axis_size("tl") + quarter) * channels
    edge = lax.ppermute(
        pool_input[:, length - SPAN :], "sp", [(i, i + 1) for i in range(blocks - 1)]
    )
    slots = slot_table(routes.T, experts, padded(capacity))
    gains = gain_rows(norm_gain)
    pooled = pool(edge, pool_input)
    group = lax.all_gather(pooled, "tl", axis=0, tiled=True)
    mix = lax.dynamic_slice(
        pool_mix, (scale, 0, quarter * channels), (1, pool_mix.shape[1], channels)
    )[0]
    mixed = lax.dot_general(mix, group, (((0,), (0,)), ((), ())), preferred_element_type=jnp.float32)
    own_scale = lax.dynamic_slice(pool_scale, (own_first,), (channels,))
    branch = (jax.nn.sigmoid(pool_gate.astype(jnp.float32)) * mixed * own_scale[:, None]).astype(jnp.bfloat16)
    branches = lax.all_gather(branch, TP, axis=0, tiled=True)
    product = lax.dot_general(
        branches, out_proj, (((0,), (0,)), ((), ())), preferred_element_type=jnp.float32
    )
    state = (residual.astype(jnp.float32) + product).astype(jnp.bfloat16)

    sent = dispatch(state, slots, blocks, capacity)
    arrived = lax.all_to_all(sent, "sp", split_axis=0, concat_axis=0, tiled=True)
    everyone = [lax.all_gather(piece, TP, axis=0, tiled=False) for piece in compact(arrived, gains)]
    activated = hidden(everyone, w_gate, w_up)
    units = [lax.all_gather(piece, TP, axis=0, tiled=False) for piece in activated]
    result = down(units, w_down, blocks, capacity)
    returned = lax.all_to_all(result, "sp", split_axis=0, concat_axis=0, tiled=True)
    weights = route_weights(routes, group_logits, expert_scores, experts // group_logits.shape[1])
    return combine(state, slots.T, weights, returned)


def solution(mesh):
    fine = Mesh(mesh.devices.reshape(mesh.devices.shape[0], 4, -1), ("sp", *TP))
    placed = (
        P(TP, "sp"),
        P(TP, "sp"),
        P(),
        P(),
        P(None, TP),
        P("sp", TP),
        P(TP),
        P("sp", None),
        P("sp", None),
        P("sp", None),
        P("sp", None, TP),
        P("sp", None, TP),
        P("sp", None, TP),
    )
    return jax.shard_map(
        per_device, mesh=fine, in_specs=placed, out_specs=P("sp", TP), check_vma=False
    )
```

```python
import jax
import jax.numpy as jnp
from jax import lax
from jax.experimental import pallas as pl
from jax.experimental.pallas import tpu as pltpu
from jax.sharding import Mesh, PartitionSpec as P

SPAN = 128
GAIN_ROWS = 16
TOGETHER = 2
AHEAD = 2
DOWN_AHEAD = 4
ROWS = 288
epsilon = 1e-06

LINE = ("tg", "yl")
SCALE = ("yl", "core")
TP = (*LINE, "core")


def vmem(mib):
    return pltpu.CompilerParams(vmem_limit_bytes=mib << 20)


def padded(rows):
    return -(-rows // 8) * 8


def pool_kernel(edge_ref, own_ref, out_ref):
    length = own_ref.shape[1]
    scale = lax.axis_index("tg")
    first = lax.axis_index("sp") * length
    own = own_ref[...].astype(jnp.float32)
    layered = jnp.concatenate([edge_ref[...].astype(jnp.float32), own], axis=1)
    chosen = None
    stride = 1
    for octave in range(4):
        layered = layered + pltpu.roll(layered, stride, 1)
        stride *= 2
        chosen = layered if chosen is None else jnp.where(scale >= octave, layered, chosen)
    window = jnp.left_shift(2, scale)
    position = first + 1 + lax.broadcasted_iota(jnp.int32, own.shape, 1)
    counted = jnp.minimum(position, window).astype(jnp.float32)
    pooled = chosen[:, SPAN : SPAN + length] / counted - own
    out_ref[...] = pooled.astype(out_ref.dtype)


def pool(edge, own):
    return pl.pallas_call(
        pool_kernel,
        out_shape=jax.ShapeDtypeStruct(own.shape, jnp.bfloat16),
        compiler_params=vmem(4),
        name="pool",
    )(edge, own)


def slot_kernel(experts, pitch, routes_ref, out_ref):
    choices, length = routes_ref.shape
    number = lax.broadcasted_iota(jnp.int32, (experts, length), 0)
    named = [(number == routes_ref[k : k + 1, :]).astype(jnp.float32) for k in range(choices)]
    earlier = lax.broadcasted_iota(jnp.int32, (length, length), 0) < lax.broadcasted_iota(
        jnp.int32, (length, length), 1
    )
    before = jnp.dot(
        sum(named).astype(jnp.bfloat16),
        jnp.where(earlier, 1.0, 0.0).astype(jnp.bfloat16),
        preferred_element_type=jnp.float32,
    )
    for k in range(choices):
        rank = jnp.sum(before * named[k], axis=0, keepdims=True).astype(jnp.int32)
        out_ref[k : k + 1, :] = routes_ref[k : k + 1, :] * pitch + rank


def slot_table(routes, experts, pitch):
    def kernel(routes_ref, out_ref):
        slot_kernel(experts, pitch, routes_ref, out_ref)

    return pl.pallas_call(
        kernel,
        out_shape=jax.ShapeDtypeStruct(routes.shape, jnp.int32),
        compiler_params=vmem(8),
        name="slots",
    )(routes)


def dispatch_kernel(pitch, own_ref, other_ref, slot_ref, out_ref):
    blocks, share, _ = out_ref.shape
    core, stride = lax.axis_index("core"), padded(share)
    first = core == 0
    own, other = own_ref[...].astype(jnp.float32), other_ref[...].astype(jnp.float32)
    state = jnp.concatenate([jnp.where(first, own, other), jnp.where(first, other, own)], axis=1)
    count = lax.broadcasted_iota(jnp.int32, (stride, own_ref.shape[0]), 0) + core * share
    place = jnp.concatenate([count + block * pitch for block in range(blocks)], axis=0)
    chosen = place == slot_ref[0:1, :]
    for k in range(1, slot_ref.shape[0]):
        chosen = chosen | (place == slot_ref[k : k + 1, :])
    spread = jnp.where(chosen, 1.0, 0.0).astype(jnp.bfloat16)
    rows = jnp.dot(spread, state.astype(jnp.bfloat16), preferred_element_type=jnp.float32)
    for block in range(blocks):
        out_ref[block] = rows[block * stride : block * stride + share].astype(out_ref.dtype)


def dispatch(own, other, slots, blocks, capacity):
    def kernel(*refs):
        dispatch_kernel(padded(capacity), *refs)

    return pl.pallas_call(
        kernel,
        out_shape=jax.ShapeDtypeStruct((blocks, capacity // 2, 2 * own.shape[1]), jnp.bfloat16),
        compiler_params=vmem(12),
        name="dispatch",
    )(own, other, slots)


def compact_kernel(arrived_ref, own_ref, other_ref, out_ref, rows_ref):
    blocks, share, width = arrived_ref.shape
    rows = blocks * share
    first = lax.axis_index("core") == 0
    for block in range(blocks):
        rows_ref[block * share : (block + 1) * share] = arrived_ref[block].astype(jnp.float32)
    own, other = own_ref[...].astype(jnp.float32), other_ref[...].astype(jnp.float32)
    rows_ref[rows:, : width // 2] = jnp.where(first, own, other)
    rows_ref[rows:, width // 2 :] = jnp.where(first, other, own)
    out_ref[...] = rows_ref[...].astype(out_ref.dtype)


def compact(arrived, own_gains, other_gains):
    shape = (arrived.shape[0] * arrived.shape[1] + GAIN_ROWS, arrived.shape[2])
    return pl.pallas_call(
        compact_kernel,
        out_shape=jax.ShapeDtypeStruct(shape, jnp.bfloat16),
        scratch_shapes=[pltpu.VMEM(shape, jnp.float32)],
        compiler_params=vmem(8),
        name="compact",
    )(arrived, own_gains, other_gains)


def tiles(rows, limit):
    size = -(-rows // -(-rows // limit) // 16) * 16
    return [(first, min(size, rows - first)) for first in range(0, rows, size)]


def begin_ahead(copies, ahead):
    for copy in sum(copies[:ahead], []):
        copy.start()


def turn_over(copies, chunk, ahead):
    for copy in copies[chunk]:
        copy.wait()
    for copy in sum(copies[chunk + ahead : chunk + ahead + 1], []):
        copy.start()


def hidden_kernel(x_hbm, gate_hbm, up_hbm, gate2_hbm, up2_hbm, out_ref, x_ref, gate_ref, up_ref, squares_ref, gate_sum, up_sum, x_sems, w_sems):
    parts, rows, width = x_ref.shape
    rows -= GAIN_ROWS
    units = gate_ref.shape[2]
    depth = TOGETHER * width
    core = lax.axis_index("core")
    copies = []
    for chunk in range(parts // TOGETHER):
        deep = pl.ds(chunk * depth, depth)
        here = [
            pltpu.make_async_copy(hbm.at[deep], ref.at[which, deep], w_sems.at[chunk, k])
            for k, (hbm, ref, which) in enumerate(
                (
                    (gate_hbm, gate_ref, core),
                    (up_hbm, up_ref, core),
                    (gate2_hbm, gate_ref, 1 - core),
                    (up2_hbm, up_ref, 1 - core),
                )
            )
        ]
        for part in range(chunk * TOGETHER, (chunk + 1) * TOGETHER):
            here.append(pltpu.make_async_copy(x_hbm.at[part], x_ref.at[part], x_sems.at[part]))
        copies.append(here)
    begin_ahead(copies, AHEAD)
    for chunk in range(len(copies)):
        turn_over(copies, chunk, AHEAD)
        mine = range(chunk * TOGETHER, (chunk + 1) * TOGETHER)
        deep = pl.ds(chunk * depth, depth)
        gains = []
        for part in mine:
            extra = x_ref[part, pl.ds(rows, GAIN_ROWS), :].astype(jnp.float32)
            gains.append(extra[0:1] + extra[1:2] + extra[2:3])
        for first, count in tiles(rows, ROWS):
            here = pl.ds(first, count)
            squares, scaled = None, []
            for part, gain in zip(mine, gains):
                state = x_ref[part, here, :].astype(jnp.float32)
                squares = state * state if squares is None else squares + state * state
                scaled.append((state * gain).astype(jnp.bfloat16))
            rows_in = jnp.concatenate(scaled, axis=1)
            if chunk == 0:
                squares_ref[here, :] = squares
            else:
                squares_ref[here, :] += squares
            for which in range(2):
                there = pl.ds(which * units, units)
                gate = jnp.dot(rows_in, gate_ref[which, deep, :], preferred_element_type=jnp.float32)
                up = jnp.dot(rows_in, up_ref[which, deep, :], preferred_element_type=jnp.float32)
                if chunk == 0:
                    gate_sum[here, there], up_sum[here, there] = gate, up
                else:
                    gate_sum[here, there] += gate
                    up_sum[here, there] += up
    for first, count in tiles(rows, ROWS):
        here = pl.ds(first, count)
        mean = jnp.sum(squares_ref[here, :], axis=1, keepdims=True) / (parts * width)
        factor = lax.rsqrt(mean + epsilon)
        gate, up = gate_sum[here, :] * factor, up_sum[here, :] * factor
        out_ref[here, :] = (jax.nn.silu(gate) * up).astype(out_ref.dtype)


def hidden(everyone, w_gate, w_up, other_gate, other_up):
    parts, extended, width = everyone.shape
    rows, units = extended - GAIN_ROWS, w_gate.shape[1]
    return pl.pallas_call(
        hidden_kernel,
        out_shape=jax.ShapeDtypeStruct((rows, 2 * units), jnp.bfloat16),
        in_specs=[pl.BlockSpec(memory_space=pltpu.HBM)] * 5,
        scratch_shapes=[
            pltpu.VMEM(everyone.shape, everyone.dtype),
            pltpu.VMEM((2, *w_gate.shape), w_gate.dtype),
            pltpu.VMEM((2, *w_up.shape), w_up.dtype),
            pltpu.VMEM((rows, width), jnp.float32),
            pltpu.VMEM((rows, 2 * units), jnp.float32),
            pltpu.VMEM((rows, 2 * units), jnp.float32),
            pltpu.SemaphoreType.DMA((parts,)),
            pltpu.SemaphoreType.DMA((parts // TOGETHER, 4)),
        ],
        name="hidden",
    )(everyone, w_gate, w_up, other_gate, other_up)


def down_kernel(u_hbm, own_hbm, other_hbm, own_out, other_out, u_ref, own_ref, other_ref, total_ref, u_sems, w_sems):
    parts, rows, units = u_ref.shape
    width = own_ref.shape[1]
    copies = []
    for part in range(parts):
        deep = pl.ds(part * units, units)
        copies.append(
            [
                pltpu.make_async_copy(own_hbm.at[deep], own_ref.at[deep], w_sems.at[part, 0]),
                pltpu.make_async_copy(other_hbm.at[deep], other_ref.at[deep], w_sems.at[part, 1]),
                pltpu.make_async_copy(u_hbm.at[part], u_ref.at[part], u_sems.at[part]),
            ]
        )
    begin_ahead(copies, DOWN_AHEAD)
    for part in range(parts):
        turn_over(copies, part, DOWN_AHEAD)
        deep = pl.ds(part * units, units)
        columns = jnp.concatenate([own_ref[deep, :], other_ref[deep, :]], axis=1)
        for first, count in tiles(rows, ROWS):
            here = pl.ds(first, count)
            product = jnp.dot(u_ref[part, here, :], columns, preferred_element_type=jnp.float32)
            if part == 0:
                total_ref[here, :] = product
            else:
                total_ref[here, :] += product
    own_out[...] = total_ref[:, :width].astype(own_out.dtype)
    other_out[...] = total_ref[:, width:].astype(other_out.dtype)


def down(everyone, own, other):
    parts, rows, units = everyone.shape
    width = own.shape[1]
    half = jax.ShapeDtypeStruct((rows, width), jnp.bfloat16)
    return pl.pallas_call(
        down_kernel,
        out_shape=[half, half],
        in_specs=[pl.BlockSpec(memory_space=pltpu.HBM)] * 3,
        scratch_shapes=[
            pltpu.VMEM(everyone.shape, everyone.dtype),
            pltpu.VMEM(own.shape, own.dtype),
            pltpu.VMEM(other.shape, other.dtype),
            pltpu.VMEM((rows, 2 * width), jnp.float32),
            pltpu.SemaphoreType.DMA((parts,)),
            pltpu.SemaphoreType.DMA((parts, 2)),
        ],
        name="down",
    )(everyone, own, other)


def unfold_kernel(own_ref, other_ref, out_ref, wide_ref):
    blocks, capacity, _ = out_ref.shape
    share = capacity // 2
    first = lax.axis_index("core") == 0
    own, other = own_ref[...].astype(jnp.float32), other_ref[...].astype(jnp.float32)
    lower, upper = jnp.where(first, own, other), jnp.where(first, other, own)
    for block in range(blocks):
        here = slice(block * share, (block + 1) * share)
        wide_ref[block, 0:share] = lower[here]
        wide_ref[block, share:capacity] = upper[here]
    out_ref[...] = wide_ref[...].astype(out_ref.dtype)


def unfold(own, other, blocks, capacity):
    shape = (blocks, capacity, own.shape[1])
    return pl.pallas_call(
        unfold_kernel,
        out_shape=jax.ShapeDtypeStruct(shape, own.dtype),
        scratch_shapes=[pltpu.VMEM(shape, jnp.float32)],
        compiler_params=vmem(8),
        name="unfold",
    )(own, other)


def combine_kernel(state_ref, slot_ref, weight_ref, returned_ref, out_ref, rows_ref):
    blocks, capacity, _ = returned_ref.shape
    pitch = padded(capacity)
    rows_ref[...] = jnp.zeros_like(rows_ref)
    for block in range(blocks):
        rows_ref[block * pitch : block * pitch + capacity] = returned_ref[block].astype(jnp.float32)
    rows = rows_ref[...].astype(jnp.bfloat16)
    place = lax.broadcasted_iota(jnp.int32, (state_ref.shape[0], blocks * pitch), 1)
    total = jnp.zeros(out_ref.shape, jnp.float32)
    for choice in range(slot_ref.shape[1]):
        pick = jnp.where(place == slot_ref[:, choice : choice + 1], 1.0, 0.0).astype(jnp.bfloat16)
        picked = jnp.dot(pick, rows, preferred_element_type=jnp.float32)
        total += weight_ref[:, choice : choice + 1] * picked
    out_ref[...] = (state_ref[...].astype(jnp.float32) + total).astype(out_ref.dtype)


def combine(state, slots, weights, returned):
    blocks, capacity, width = returned.shape
    return pl.pallas_call(
        combine_kernel,
        out_shape=jax.ShapeDtypeStruct(state.shape, jnp.bfloat16),
        scratch_shapes=[pltpu.VMEM((blocks * padded(capacity), width), jnp.float32)],
        compiler_params=vmem(12),
        name="combine",
    )(state, slots, weights, returned)


def route_weights(routes, group_logits, expert_scores, per_group):
    raised = jnp.exp(group_logits)
    group_prob = raised / jnp.sum(raised, axis=1, keepdims=True)
    owning_group = routes // per_group
    groups_iota = jnp.arange(group_logits.shape[1], dtype=jnp.int32)
    picked = jnp.sum(
        jnp.where(owning_group[:, :, None] == groups_iota[None, None, :], group_prob[:, None, :], 0.0),
        axis=2,
    )
    lifted = jnp.exp(expert_scores)
    return picked * lifted / jnp.sum(lifted, axis=1, keepdims=True)


def to_travel(values):
    wide = values.astype(jnp.float32)
    root = jnp.sqrt(jnp.abs(wide))
    return jnp.where(wide < 0, -root, root).astype(jnp.float16)


def from_travel(roots):
    wide = roots.astype(jnp.float32)
    return (wide * jnp.abs(wide)).astype(jnp.bfloat16)


def to_line(values):
    return from_travel(lax.all_gather(to_travel(values), LINE, axis=0, tiled=False))


def swap(values):
    return lax.ppermute(values, "core", [(0, 1), (1, 0)])


def gain_rows(gain):
    row = lax.broadcasted_iota(jnp.int32, (GAIN_ROWS, gain.shape[0]), 0)
    rows, rest = jnp.zeros(row.shape, jnp.float32), gain[None, :]
    for k in range(3):
        head = lax.reduce_precision(rest, 8, 7)
        rows = jnp.where(row == k, head, rows)
        rest = rest - head
    return rows.astype(jnp.bfloat16)


def per_device(
    pool_input,
    pool_gate,
    pool_mix,
    pool_scale,
    out_proj,
    residual,
    norm_gain,
    routes,
    group_logits,
    expert_scores,
    w_gate,
    w_up,
    w_down,
):
    channels, length = pool_input.shape
    blocks = lax.axis_size("sp")
    experts = blocks * w_gate.shape[0]
    capacity = 3 * routes.shape[1] * length // (2 * experts)
    scale, quarter = lax.axis_index("tg"), lax.axis_index(SCALE)
    own_first = (scale * lax.axis_size(SCALE) + quarter) * channels
    edge = lax.ppermute(
        pool_input[:, length - SPAN :], "sp", [(i, i + 1) for i in range(blocks - 1)]
    )
    slots = slot_table(routes.T, experts, padded(capacity))
    gains = gain_rows(norm_gain)
    pooled = pool(edge, pool_input)
    group = lax.all_gather(pooled, SCALE, axis=0, tiled=True)
    mix = lax.dynamic_slice(
        pool_mix, (scale, 0, quarter * channels), (1, pool_mix.shape[1], channels)
    )[0]
    mixed = lax.dot_general(mix, group, (((0,), (0,)), ((), ())), preferred_element_type=jnp.float32)
    own_scale = lax.dynamic_slice(pool_scale, (own_first,), (channels,))
    branch = (jax.nn.sigmoid(pool_gate.astype(jnp.float32)) * mixed * own_scale[:, None]).astype(jnp.bfloat16)
    branches = lax.all_gather(branch, TP, axis=0, tiled=True)
    product = lax.dot_general(
        branches, out_proj, (((0,), (0,)), ((), ())), preferred_element_type=jnp.float32
    )
    state = (residual.astype(jnp.float32) + product).astype(jnp.bfloat16)

    other_state = swap(state)
    sent = dispatch(state, other_state, slots, blocks, capacity)
    w_gate, w_up, w_down = w_gate[0], w_up[0], w_down[0]
    other_gate, other_up, other_down, other_gains = swap(w_gate), swap(w_up), swap(w_down), swap(gains)
    arrived = lax.all_to_all(sent, "sp", split_axis=0, concat_axis=0, tiled=True)
    everyone = to_line(compact(arrived, gains, other_gains))
    activated = hidden(everyone, w_gate, w_up, other_gate, other_up)
    own_result, other_result = down(to_line(activated), w_down, other_down)
    result = unfold(own_result, swap(other_result), blocks, capacity)
    returned = lax.all_to_all(result, "sp", split_axis=0, concat_axis=0, tiled=True)
    weights = route_weights(routes, group_logits, expert_scores, experts // group_logits.shape[1])
    return combine(state, slots.T, weights, returned)


def solution(mesh):
    fine = Mesh(mesh.devices.reshape(mesh.devices.shape[0], 4, -1, 2), ("sp", *TP))
    placed = (
        P(TP, "sp"),
        P(TP, "sp"),
        P(),
        P(),
        P(None, TP),
        P("sp", TP),
        P(TP),
        P("sp", None),
        P("sp", None),
        P("sp", None),
        P("sp", None, TP),
        P("sp", None, TP),
        P("sp", None, TP),
    )
    return jax.shard_map(
        per_device, mesh=fine, in_specs=placed, out_specs=P("sp", TP), check_vma=False
    )
```

```python
import jax
import jax.numpy as jnp
from jax import lax
from jax.experimental import pallas as pl
from jax.experimental.pallas import tpu as pltpu
from jax.sharding import Mesh, PartitionSpec as P

SPAN = 128
GAIN_ROWS = 16
TOGETHER = 2
AHEAD = 2
DOWN_AHEAD = 4
HIDDEN_MIB = 20
DOWN_MIB = 16
ROWS = 288
epsilon = 1e-06

LINE = ("tg", "yl")
SCALE = ("yl", "core")
TP = (*LINE, "core")


def vmem(mib):
    return pltpu.CompilerParams(vmem_limit_bytes=mib << 20)


def padded(rows):
    return -(-rows // 8) * 8


def pool_kernel(edge_ref, own_ref, gain_ref, out_ref):
    length = own_ref.shape[1]
    scale = lax.axis_index("tg")
    first = lax.axis_index("sp") * length
    own = own_ref[...].astype(jnp.float32)
    layered = jnp.concatenate([edge_ref[...].astype(jnp.float32), own], axis=1)
    chosen = None
    stride = 1
    for octave in range(4):
        layered = layered + pltpu.roll(layered, stride, 1)
        stride *= 2
        chosen = layered if chosen is None else jnp.where(scale >= octave, layered, chosen)
    window = jnp.left_shift(2, scale)
    position = first + 1 + lax.broadcasted_iota(jnp.int32, own.shape, 1)
    counted = jnp.minimum(position, window).astype(jnp.float32)
    pooled = chosen[:, SPAN : SPAN + length] / counted - own
    out_ref[:, :length] = pooled.astype(out_ref.dtype)
    out_ref[:, length:] = jnp.zeros((own.shape[0], SPAN), out_ref.dtype)
    out_ref[0:GAIN_ROWS, length:] = gain_ref[...]


def pool(edge, own, gains):
    channels, length = own.shape
    return pl.pallas_call(
        pool_kernel,
        out_shape=jax.ShapeDtypeStruct((channels, length + SPAN), jnp.bfloat16),
        compiler_params=vmem(4),
        name="pool",
    )(edge, own, gains)


def slot_kernel(experts, pitch, routes_ref, out_ref):
    choices, length = routes_ref.shape
    number = lax.broadcasted_iota(jnp.int32, (experts, length), 0)
    named = [(number == routes_ref[k : k + 1, :]).astype(jnp.float32) for k in range(choices)]
    earlier = lax.broadcasted_iota(jnp.int32, (length, length), 0) < lax.broadcasted_iota(
        jnp.int32, (length, length), 1
    )
    before = jnp.dot(
        sum(named).astype(jnp.bfloat16),
        jnp.where(earlier, 1.0, 0.0).astype(jnp.bfloat16),
        preferred_element_type=jnp.float32,
    )
    for k in range(choices):
        rank = jnp.sum(before * named[k], axis=0, keepdims=True).astype(jnp.int32)
        out_ref[k : k + 1, :] = routes_ref[k : k + 1, :] * pitch + rank


def slot_table(routes, experts, pitch):
    def kernel(routes_ref, out_ref):
        slot_kernel(experts, pitch, routes_ref, out_ref)

    return pl.pallas_call(
        kernel,
        out_shape=jax.ShapeDtypeStruct(routes.shape, jnp.int32),
        compiler_params=vmem(8),
        name="slots",
    )(routes)


def dispatch_kernel(pitch, own_ref, other_ref, slot_ref, out_ref):
    blocks, share, _ = out_ref.shape
    core, stride = lax.axis_index("core"), padded(share)
    first = core == 0
    own, other = own_ref[...].astype(jnp.float32), other_ref[...].astype(jnp.float32)
    state = jnp.concatenate([jnp.where(first, own, other), jnp.where(first, other, own)], axis=1)
    count = lax.broadcasted_iota(jnp.int32, (stride, own_ref.shape[0]), 0) + core * share
    place = jnp.concatenate([count + block * pitch for block in range(blocks)], axis=0)
    chosen = place == slot_ref[0:1, :]
    for k in range(1, slot_ref.shape[0]):
        chosen = chosen | (place == slot_ref[k : k + 1, :])
    spread = jnp.where(chosen, 1.0, 0.0).astype(jnp.bfloat16)
    rows = jnp.dot(spread, state.astype(jnp.bfloat16), preferred_element_type=jnp.float32)
    for block in range(blocks):
        out_ref[block] = rows[block * stride : block * stride + share].astype(out_ref.dtype)


def dispatch(own, other, slots, blocks, capacity):
    def kernel(*refs):
        dispatch_kernel(padded(capacity), *refs)

    return pl.pallas_call(
        kernel,
        out_shape=jax.ShapeDtypeStruct((blocks, capacity // 2, 2 * own.shape[1]), jnp.bfloat16),
        compiler_params=vmem(12),
        name="dispatch",
    )(own, other, slots)


def compact_kernel(arrived_ref, own_ref, other_ref, out_ref, rows_ref):
    blocks, share, width = arrived_ref.shape
    rows = blocks * share
    first = lax.axis_index("core") == 0
    for block in range(blocks):
        rows_ref[block * share : (block + 1) * share] = arrived_ref[block].astype(jnp.float32)
    own, other = own_ref[...].astype(jnp.float32), other_ref[...].astype(jnp.float32)
    rows_ref[rows:, : width // 2] = jnp.where(first, own, other)
    rows_ref[rows:, width // 2 :] = jnp.where(first, other, own)
    out_ref[...] = rows_ref[...].astype(out_ref.dtype)


def compact(arrived, own_gains, other_gains):
    shape = (arrived.shape[0] * arrived.shape[1] + GAIN_ROWS, arrived.shape[2])
    return pl.pallas_call(
        compact_kernel,
        out_shape=jax.ShapeDtypeStruct(shape, jnp.bfloat16),
        scratch_shapes=[pltpu.VMEM(shape, jnp.float32)],
        compiler_params=vmem(8),
        name="compact",
    )(arrived, own_gains, other_gains)


def tiles(rows, limit):
    size = -(-rows // -(-rows // limit) // 16) * 16
    return [(first, min(size, rows - first)) for first in range(0, rows, size)]


def begin_ahead(copies, ahead):
    for copy in sum(copies[:ahead], []):
        copy.start()


def turn_over(copies, chunk, ahead):
    for copy in copies[chunk]:
        copy.wait()
    for copy in sum(copies[chunk + ahead : chunk + ahead + 1], []):
        copy.start()


def hidden_kernel(x_ref, gate_ref, up_ref, gate2_hbm, up2_hbm, out_ref, gate2_ref, up2_ref, squares_ref, *refs):
    sums, w_sems = refs[:4], refs[4]
    parts, rows, width = x_ref.shape
    rows -= GAIN_ROWS
    units = gate_ref.shape[1]
    depth = TOGETHER * width
    chunks = parts // TOGETHER
    copies = []
    for chunk in range(chunks):
        deep = pl.ds(chunk * depth, depth)
        copies.append(
            [
                pltpu.make_async_copy(hbm.at[deep], ref.at[deep], w_sems.at[chunk, k])
                for k, (hbm, ref) in enumerate(((gate2_hbm, gate2_ref), (up2_hbm, up2_ref)))
            ]
        )
    begin_ahead(copies, AHEAD)
    for chunk in range(chunks):
        turn_over(copies, chunk, AHEAD)
        mine = range(chunk * TOGETHER, (chunk + 1) * TOGETHER)
        deep = pl.ds(chunk * depth, depth)
        gains = []
        for part in mine:
            extra = x_ref[part, pl.ds(rows, GAIN_ROWS), :].astype(jnp.float32)
            gains.append(extra[0:1] + extra[1:2] + extra[2:3])
        for first, count in tiles(rows, ROWS):
            here = pl.ds(first, count)
            squares, scaled = None, []
            for part, gain in zip(mine, gains):
                state = x_ref[part, here, :].astype(jnp.float32)
                squares = state * state if squares is None else squares + state * state
                scaled.append((state * gain).astype(jnp.bfloat16))
            rows_in = jnp.concatenate(scaled, axis=1)
            if chunk == 0:
                squares_ref[here, :] = squares
            else:
                squares_ref[here, :] += squares
            for total_ref, weight_ref in zip(sums, (gate_ref, up_ref, gate2_ref, up2_ref)):
                product = jnp.dot(rows_in, weight_ref[deep, :], preferred_element_type=jnp.float32)
                if chunk == 0:
                    total_ref[here, :] = product
                else:
                    total_ref[here, :] += product
    lower = lax.axis_index("core") == 0
    for first, count in tiles(rows, ROWS):
        here = pl.ds(first, count)
        mean = jnp.sum(squares_ref[here, :], axis=1, keepdims=True) / (parts * width)
        factor = lax.rsqrt(mean + epsilon)
        gate, up, gate2, up2 = [total_ref[here, :] * factor for total_ref in sums]
        own, other = jax.nn.silu(gate) * up, jax.nn.silu(gate2) * up2
        out_ref[here, :units] = jnp.where(lower, own, other).astype(out_ref.dtype)
        out_ref[here, units:] = jnp.where(lower, other, own).astype(out_ref.dtype)


def hidden(everyone, w_gate, w_up, other_gate, other_up):
    parts, extended, width = everyone.shape
    rows, units = extended - GAIN_ROWS, w_gate.shape[1]
    hbm, near = pl.BlockSpec(memory_space=pltpu.HBM), pl.BlockSpec(memory_space=pltpu.VMEM)
    return pl.pallas_call(
        hidden_kernel,
        out_shape=jax.ShapeDtypeStruct((rows, 2 * units), jnp.bfloat16),
        in_specs=[near, near, near, hbm, hbm],
        scratch_shapes=[
            pltpu.VMEM(w_gate.shape, w_gate.dtype),
            pltpu.VMEM(w_up.shape, w_up.dtype),
            pltpu.VMEM((rows, width), jnp.float32),
            *[pltpu.VMEM((rows, units), jnp.float32)] * 4,
            pltpu.SemaphoreType.DMA((parts // TOGETHER, 2)),
        ],
        compiler_params=vmem(HIDDEN_MIB),
        name="hidden",
    )(everyone, w_gate, w_up, other_gate, other_up)


def down_kernel(u_ref, own_hbm, other_hbm, own_out, other_out, own_ref, other_ref, total_ref, w_sems):
    parts, rows, units = u_ref.shape
    width = own_ref.shape[1]
    copies = []
    for part in range(parts):
        deep = pl.ds(part * units, units)
        copies.append(
            [
                pltpu.make_async_copy(own_hbm.at[deep], own_ref.at[deep], w_sems.at[part, 0]),
                pltpu.make_async_copy(other_hbm.at[deep], other_ref.at[deep], w_sems.at[part, 1]),
            ]
        )
    begin_ahead(copies, DOWN_AHEAD)
    for part in range(parts):
        turn_over(copies, part, DOWN_AHEAD)
        deep = pl.ds(part * units, units)
        columns = jnp.concatenate([own_ref[deep, :], other_ref[deep, :]], axis=1)
        for first, count in tiles(rows, ROWS):
            here = pl.ds(first, count)
            product = jnp.dot(u_ref[part, here, :], columns, preferred_element_type=jnp.float32)
            if part == 0:
                total_ref[here, :] = product
            else:
                total_ref[here, :] += product
    own_out[...] = total_ref[:, :width].astype(own_out.dtype)
    other_out[...] = total_ref[:, width:].astype(other_out.dtype)


def down(everyone, own, other):
    parts, rows, units = everyone.shape
    width = own.shape[1]
    half = jax.ShapeDtypeStruct((rows, width), jnp.bfloat16)
    hbm, near = pl.BlockSpec(memory_space=pltpu.HBM), pl.BlockSpec(memory_space=pltpu.VMEM)
    return pl.pallas_call(
        down_kernel,
        out_shape=[half, half],
        in_specs=[near, hbm, hbm],
        scratch_shapes=[
            pltpu.VMEM(own.shape, own.dtype),
            pltpu.VMEM(other.shape, other.dtype),
            pltpu.VMEM((rows, 2 * width), jnp.float32),
            pltpu.SemaphoreType.DMA((parts, 2)),
        ],
        compiler_params=vmem(DOWN_MIB),
        name="down",
    )(everyone, own, other)


def unfold_kernel(own_ref, other_ref, out_ref, wide_ref):
    blocks, capacity, _ = out_ref.shape
    share = capacity // 2
    first = lax.axis_index("core") == 0
    own, other = own_ref[...].astype(jnp.float32), other_ref[...].astype(jnp.float32)
    lower, upper = jnp.where(first, own, other), jnp.where(first, other, own)
    for block in range(blocks):
        here = slice(block * share, (block + 1) * share)
        wide_ref[block, 0:share] = lower[here]
        wide_ref[block, share:capacity] = upper[here]
    out_ref[...] = wide_ref[...].astype(out_ref.dtype)


def unfold(own, other, blocks, capacity):
    shape = (blocks, capacity, own.shape[1])
    return pl.pallas_call(
        unfold_kernel,
        out_shape=jax.ShapeDtypeStruct(shape, own.dtype),
        scratch_shapes=[pltpu.VMEM(shape, jnp.float32)],
        compiler_params=vmem(8),
        name="unfold",
    )(own, other)


def combine_kernel(state_ref, slot_ref, weight_ref, returned_ref, out_ref, rows_ref):
    blocks, capacity, _ = returned_ref.shape
    pitch = padded(capacity)
    rows_ref[...] = jnp.zeros_like(rows_ref)
    for block in range(blocks):
        rows_ref[block * pitch : block * pitch + capacity] = returned_ref[block].astype(jnp.float32)
    rows = rows_ref[...].astype(jnp.bfloat16)
    place = lax.broadcasted_iota(jnp.int32, (state_ref.shape[0], blocks * pitch), 1)
    total = jnp.zeros(out_ref.shape, jnp.float32)
    for choice in range(slot_ref.shape[1]):
        pick = jnp.where(place == slot_ref[:, choice : choice + 1], 1.0, 0.0).astype(jnp.bfloat16)
        picked = jnp.dot(pick, rows, preferred_element_type=jnp.float32)
        total += weight_ref[:, choice : choice + 1] * picked
    out_ref[...] = (state_ref[...].astype(jnp.float32) + total).astype(out_ref.dtype)


def combine(state, slots, weights, returned):
    blocks, capacity, width = returned.shape
    return pl.pallas_call(
        combine_kernel,
        out_shape=jax.ShapeDtypeStruct(state.shape, jnp.bfloat16),
        scratch_shapes=[pltpu.VMEM((blocks * padded(capacity), width), jnp.float32)],
        compiler_params=vmem(12),
        name="combine",
    )(state, slots, weights, returned)


def route_weights(routes, group_logits, expert_scores, per_group):
    raised = jnp.exp(group_logits)
    group_prob = raised / jnp.sum(raised, axis=1, keepdims=True)
    owning_group = routes // per_group
    groups_iota = jnp.arange(group_logits.shape[1], dtype=jnp.int32)
    picked = jnp.sum(
        jnp.where(owning_group[:, :, None] == groups_iota[None, None, :], group_prob[:, None, :], 0.0),
        axis=2,
    )
    lifted = jnp.exp(expert_scores)
    return picked * lifted / jnp.sum(lifted, axis=1, keepdims=True)


def to_travel(values):
    wide = values.astype(jnp.float32)
    root = jnp.sqrt(jnp.abs(wide))
    return jnp.where(wide < 0, -root, root).astype(jnp.float16)


def from_travel(roots):
    wide = roots.astype(jnp.float32)
    return (wide * jnp.abs(wide)).astype(jnp.bfloat16)


def to_line(values):
    return from_travel(lax.all_gather(to_travel(values), LINE, axis=0, tiled=False))


def swap(values):
    return lax.ppermute(values, "core", [(0, 1), (1, 0)])


def gain_rows(gain):
    row = lax.broadcasted_iota(jnp.int32, (GAIN_ROWS, gain.shape[0]), 0)
    rows, rest = jnp.zeros(row.shape, jnp.float32), gain[None, :]
    for k in range(3):
        head = lax.reduce_precision(rest, 8, 7)
        rows = jnp.where(row == k, head, rows)
        rest = rest - head
    return rows.astype(jnp.bfloat16)


def per_device(
    pool_input,
    pool_gate,
    pool_mix,
    pool_scale,
    out_proj,
    residual,
    norm_gain,
    routes,
    group_logits,
    expert_scores,
    w_gate,
    w_up,
    w_down,
):
    channels, length = pool_input.shape
    blocks = lax.axis_size("sp")
    experts = blocks * w_gate.shape[0]
    capacity = 3 * routes.shape[1] * length // (2 * experts)
    scale, quarter = lax.axis_index("tg"), lax.axis_index(SCALE)
    core = lax.axis_index("core")
    own_first = (scale * lax.axis_size(SCALE) + quarter) * channels
    edge = lax.ppermute(
        pool_input[:, length - SPAN :], "sp", [(i, i + 1) for i in range(blocks - 1)]
    )
    slots = slot_table(routes.T, experts, padded(capacity))
    gains = gain_rows(norm_gain)
    pooled = pool(edge, pool_input, gains)
    group = lax.all_gather(pooled, SCALE, axis=0, tiled=True)
    mix = lax.dynamic_slice(
        pool_mix, (scale, 0, quarter * channels), (1, pool_mix.shape[1], channels)
    )[0]
    mixed = lax.dot_general(mix, group[:, :length], (((0,), (0,)), ((), ())), preferred_element_type=jnp.float32)
    other_gains = lax.dynamic_slice(group, ((quarter + 1 - 2 * core) * channels, length), (GAIN_ROWS, SPAN))
    own_scale = lax.dynamic_slice(pool_scale, (own_first,), (channels,))
    branch = (jax.nn.sigmoid(pool_gate.astype(jnp.float32)) * mixed * own_scale[:, None]).astype(jnp.bfloat16)
    branches = lax.all_gather(branch, LINE, axis=0, tiled=True)
    proj = out_proj.reshape(lax.axis_size(LINE), 2, channels, -1)
    own_proj, other_proj = lax.optimization_barrier(
        tuple(lax.dynamic_index_in_dim(proj, which, 1, keepdims=False) for which in (core, 1 - core))
    )
    swapped, other_gains = lax.optimization_barrier((swap(branches), other_gains))
    product = sum(
        lax.dot_general(
            rows,
            columns.reshape(rows.shape[0], -1),
            (((0,), (0,)), ((), ())),
            preferred_element_type=jnp.float32,
        )
        for rows, columns in ((branches, own_proj), (swapped, other_proj))
    )
    state = (residual.astype(jnp.float32) + product).astype(jnp.bfloat16)

    other_state = swap(state)
    sent = dispatch(state, other_state, slots, blocks, capacity)
    w_gate, w_up, w_down = w_gate[0], w_up[0], w_down[0]
    other_gate, other_up, other_down = swap(w_gate), swap(w_up), swap(w_down)
    arrived = lax.all_to_all(sent, "sp", split_axis=0, concat_axis=0, tiled=True)
    everyone = to_line(compact(arrived, gains, other_gains))
    activated = hidden(everyone, w_gate, w_up, other_gate, other_up)
    own_result, other_result = down(to_line(activated), w_down, other_down)
    result = unfold(own_result, swap(other_result), blocks, capacity)
    result, routes, group_logits, expert_scores = lax.optimization_barrier(
        (result, routes, group_logits, expert_scores)
    )
    weights = route_weights(routes, group_logits, expert_scores, experts // group_logits.shape[1])
    returned = lax.all_to_all(result, "sp", split_axis=0, concat_axis=0, tiled=True)
    return combine(state, slots.T, weights, returned)


def solution(mesh):
    fine = Mesh(mesh.devices.reshape(mesh.devices.shape[0], 4, -1, 2), ("sp", *TP))
    placed = (
        P(TP, "sp"),
        P(TP, "sp"),
        P(),
        P(),
        P(None, TP),
        P("sp", TP),
        P(TP),
        P("sp", None),
        P("sp", None),
        P("sp", None),
        P("sp", None, TP),
        P("sp", None, TP),
        P("sp", None, TP),
    )
    return jax.shard_map(
        per_device, mesh=fine, in_specs=placed, out_specs=P("sp", TP), check_vma=False
    )
```

```python
import jax
import jax.numpy as jnp
from jax import lax
from jax.experimental import pallas as pl
from jax.experimental.pallas import tpu as pltpu
from jax.sharding import Mesh, PartitionSpec as P

SPAN = 128
GAIN_ROWS = 16
TOGETHER = 2
AHEAD = 2
DOWN_AHEAD = 4
HIDDEN_MIB = 20
DOWN_MIB = 16
ROWS = 288
epsilon = 1e-06

LINE = ("tg", "yl")
SCALE = ("yl", "core")
TP = (*LINE, "core")


def vmem(mib):
    return pltpu.CompilerParams(vmem_limit_bytes=mib << 20)


def padded(rows):
    return -(-rows // 8) * 8


def pool_kernel(edge_ref, own_ref, gain_ref, out_ref):
    length = own_ref.shape[1]
    scale = lax.axis_index("tg")
    first = lax.axis_index("sp") * length
    own = own_ref[...].astype(jnp.float32)
    layered = jnp.concatenate([edge_ref[...].astype(jnp.float32), own], axis=1)
    chosen = None
    stride = 1
    for octave in range(4):
        layered = layered + pltpu.roll(layered, stride, 1)
        stride *= 2
        chosen = layered if chosen is None else jnp.where(scale >= octave, layered, chosen)
    window = jnp.left_shift(2, scale)
    position = first + 1 + lax.broadcasted_iota(jnp.int32, own.shape, 1)
    counted = jnp.minimum(position, window).astype(jnp.float32)
    pooled = chosen[:, SPAN : SPAN + length] / counted - own
    out_ref[:, :length] = pooled.astype(out_ref.dtype)
    out_ref[:, length:] = jnp.zeros((own.shape[0], SPAN), out_ref.dtype)
    out_ref[0:GAIN_ROWS, length:] = gain_ref[...]


def pool(edge, own, gains):
    channels, length = own.shape
    return pl.pallas_call(
        pool_kernel,
        out_shape=jax.ShapeDtypeStruct((channels, length + SPAN), jnp.bfloat16),
        compiler_params=vmem(4),
        name="pool",
    )(edge, own, gains)


def slot_kernel(experts, pitch, routes_ref, out_ref):
    choices, length = routes_ref.shape
    number = lax.broadcasted_iota(jnp.int32, (experts, length), 0)
    named = [(number == routes_ref[k : k + 1, :]).astype(jnp.float32) for k in range(choices)]
    earlier = lax.broadcasted_iota(jnp.int32, (length, length), 0) < lax.broadcasted_iota(
        jnp.int32, (length, length), 1
    )
    before = jnp.dot(
        sum(named).astype(jnp.bfloat16),
        jnp.where(earlier, 1.0, 0.0).astype(jnp.bfloat16),
        preferred_element_type=jnp.float32,
    )
    for k in range(choices):
        rank = jnp.sum(before * named[k], axis=0, keepdims=True).astype(jnp.int32)
        out_ref[k : k + 1, :] = routes_ref[k : k + 1, :] * pitch + rank


def slot_table(routes, experts, pitch):
    def kernel(routes_ref, out_ref):
        slot_kernel(experts, pitch, routes_ref, out_ref)

    return pl.pallas_call(
        kernel,
        out_shape=jax.ShapeDtypeStruct(routes.shape, jnp.int32),
        compiler_params=vmem(8),
        name="slots",
    )(routes)


def dispatch_kernel(pitch, own_ref, other_ref, slot_ref, out_ref):
    blocks, share, _ = out_ref.shape
    core, stride = lax.axis_index("core"), padded(share)
    first = core == 0
    own, other = own_ref[...].astype(jnp.float32), other_ref[...].astype(jnp.float32)
    state = jnp.concatenate([jnp.where(first, own, other), jnp.where(first, other, own)], axis=1)
    count = lax.broadcasted_iota(jnp.int32, (stride, own_ref.shape[0]), 0) + core * share
    place = jnp.concatenate([count + block * pitch for block in range(blocks)], axis=0)
    chosen = place == slot_ref[0:1, :]
    for k in range(1, slot_ref.shape[0]):
        chosen = chosen | (place == slot_ref[k : k + 1, :])
    spread = jnp.where(chosen, 1.0, 0.0).astype(jnp.bfloat16)
    rows = jnp.dot(spread, state.astype(jnp.bfloat16), preferred_element_type=jnp.float32)
    for block in range(blocks):
        out_ref[block] = rows[block * stride : block * stride + share].astype(out_ref.dtype)


def dispatch(own, other, slots, blocks, capacity):
    def kernel(*refs):
        dispatch_kernel(padded(capacity), *refs)

    return pl.pallas_call(
        kernel,
        out_shape=jax.ShapeDtypeStruct((blocks, capacity // 2, 2 * own.shape[1]), jnp.bfloat16),
        compiler_params=vmem(12),
        name="dispatch",
    )(own, other, slots)


def compact_kernel(arrived_ref, own_ref, other_ref, out_ref, rows_ref):
    blocks, share, width = arrived_ref.shape
    rows = blocks * share
    first = lax.axis_index("core") == 0
    for block in range(blocks):
        rows_ref[block * share : (block + 1) * share] = arrived_ref[block].astype(jnp.float32)
    own, other = own_ref[...].astype(jnp.float32), other_ref[...].astype(jnp.float32)
    rows_ref[rows:, : width // 2] = jnp.where(first, own, other)
    rows_ref[rows:, width // 2 :] = jnp.where(first, other, own)
    out_ref[...] = rows_ref[...].astype(out_ref.dtype)


def compact(arrived, own_gains, other_gains):
    shape = (arrived.shape[0] * arrived.shape[1] + GAIN_ROWS, arrived.shape[2])
    return pl.pallas_call(
        compact_kernel,
        out_shape=jax.ShapeDtypeStruct(shape, jnp.bfloat16),
        scratch_shapes=[pltpu.VMEM(shape, jnp.float32)],
        compiler_params=vmem(8),
        name="compact",
    )(arrived, own_gains, other_gains)


def tiles(rows, limit):
    size = -(-rows // -(-rows // limit) // 16) * 16
    return [(first, min(size, rows - first)) for first in range(0, rows, size)]


def begin_ahead(copies, ahead):
    for copy in sum(copies[:ahead], []):
        copy.start()


def turn_over(copies, chunk, ahead):
    for copy in copies[chunk]:
        copy.wait()
    for copy in sum(copies[chunk + ahead : chunk + ahead + 1], []):
        copy.start()


def hidden_kernel(x_ref, gate_ref, up_ref, gate2_hbm, up2_hbm, out_ref, gate2_ref, up2_ref, squares_ref, *refs):
    sums, w_sems = refs[:4], refs[4]
    parts, rows, width = x_ref.shape
    rows -= GAIN_ROWS
    units = gate_ref.shape[1]
    depth = TOGETHER * width
    chunks = parts // TOGETHER
    copies = []
    for chunk in range(chunks):
        deep = pl.ds(chunk * depth, depth)
        copies.append(
            [
                pltpu.make_async_copy(hbm.at[deep], ref.at[deep], w_sems.at[chunk, k])
                for k, (hbm, ref) in enumerate(((gate2_hbm, gate2_ref), (up2_hbm, up2_ref)))
            ]
        )
    begin_ahead(copies, AHEAD)
    for chunk in range(chunks):
        turn_over(copies, chunk, AHEAD)
        mine = range(chunk * TOGETHER, (chunk + 1) * TOGETHER)
        deep = pl.ds(chunk * depth, depth)
        gains = []
        for part in mine:
            extra = x_ref[part, pl.ds(rows, GAIN_ROWS), :].astype(jnp.float32)
            gains.append(extra[0:1] + extra[1:2] + extra[2:3])
        for first, count in tiles(rows, ROWS):
            here = pl.ds(first, count)
            squares, scaled = None, []
            for part, gain in zip(mine, gains):
                state = x_ref[part, here, :].astype(jnp.float32)
                squares = state * state if squares is None else squares + state * state
                scaled.append((state * gain).astype(jnp.bfloat16))
            rows_in = jnp.concatenate(scaled, axis=1)
            if chunk == 0:
                squares_ref[here, :] = squares
            else:
                squares_ref[here, :] += squares
            for total_ref, weight_ref in zip(sums, (gate_ref, up_ref, gate2_ref, up2_ref)):
                product = jnp.dot(rows_in, weight_ref[deep, :], preferred_element_type=jnp.float32)
                if chunk == 0:
                    total_ref[here, :] = product
                else:
                    total_ref[here, :] += product
    lower = lax.axis_index("core") == 0
    for first, count in tiles(rows, ROWS):
        here = pl.ds(first, count)
        mean = jnp.sum(squares_ref[here, :], axis=1, keepdims=True) / (parts * width)
        factor = lax.rsqrt(mean + epsilon)
        gate, up, gate2, up2 = [total_ref[here, :] * factor for total_ref in sums]
        own, other = jax.nn.silu(gate) * up, jax.nn.silu(gate2) * up2
        out_ref[here, :units] = jnp.where(lower, own, other).astype(out_ref.dtype)
        out_ref[here, units:] = jnp.where(lower, other, own).astype(out_ref.dtype)


def hidden(everyone, w_gate, w_up, other_gate, other_up):
    parts, extended, width = everyone.shape
    rows, units = extended - GAIN_ROWS, w_gate.shape[1]
    hbm, near = pl.BlockSpec(memory_space=pltpu.HBM), pl.BlockSpec(memory_space=pltpu.VMEM)
    return pl.pallas_call(
        hidden_kernel,
        out_shape=jax.ShapeDtypeStruct((rows, 2 * units), jnp.bfloat16),
        in_specs=[near, near, near, hbm, hbm],
        scratch_shapes=[
            pltpu.VMEM(w_gate.shape, w_gate.dtype),
            pltpu.VMEM(w_up.shape, w_up.dtype),
            pltpu.VMEM((rows, width), jnp.float32),
            *[pltpu.VMEM((rows, units), jnp.float32)] * 4,
            pltpu.SemaphoreType.DMA((parts // TOGETHER, 2)),
        ],
        compiler_params=vmem(HIDDEN_MIB),
        name="hidden",
    )(everyone, w_gate, w_up, other_gate, other_up)


def down_kernel(u_ref, own_hbm, other_hbm, own_out, other_out, own_ref, other_ref, total_ref, w_sems):
    parts, rows, units = u_ref.shape
    width = own_ref.shape[1]
    copies = []
    for part in range(parts):
        deep = pl.ds(part * units, units)
        copies.append(
            [
                pltpu.make_async_copy(own_hbm.at[deep], own_ref.at[deep], w_sems.at[part, 0]),
                pltpu.make_async_copy(other_hbm.at[deep], other_ref.at[deep], w_sems.at[part, 1]),
            ]
        )
    begin_ahead(copies, DOWN_AHEAD)
    for part in range(parts):
        turn_over(copies, part, DOWN_AHEAD)
        deep = pl.ds(part * units, units)
        columns = jnp.concatenate([own_ref[deep, :], other_ref[deep, :]], axis=1)
        for first, count in tiles(rows, ROWS):
            here = pl.ds(first, count)
            product = jnp.dot(u_ref[part, here, :], columns, preferred_element_type=jnp.float32)
            if part == 0:
                total_ref[here, :] = product
            else:
                total_ref[here, :] += product
    own_out[...] = total_ref[:, :width].astype(own_out.dtype)
    other_out[...] = total_ref[:, width:].astype(other_out.dtype)


def down(everyone, own, other):
    parts, rows, units = everyone.shape
    width = own.shape[1]
    half = jax.ShapeDtypeStruct((rows, width), jnp.bfloat16)
    hbm, near = pl.BlockSpec(memory_space=pltpu.HBM), pl.BlockSpec(memory_space=pltpu.VMEM)
    return pl.pallas_call(
        down_kernel,
        out_shape=[half, half],
        in_specs=[near, hbm, hbm],
        scratch_shapes=[
            pltpu.VMEM(own.shape, own.dtype),
            pltpu.VMEM(other.shape, other.dtype),
            pltpu.VMEM((rows, 2 * width), jnp.float32),
            pltpu.SemaphoreType.DMA((parts, 2)),
        ],
        compiler_params=vmem(DOWN_MIB),
        name="down",
    )(everyone, own, other)


def unfold_kernel(own_ref, other_ref, out_ref, wide_ref):
    blocks, capacity, _ = out_ref.shape
    share = capacity // 2
    first = lax.axis_index("core") == 0
    own, other = own_ref[...].astype(jnp.float32), other_ref[...].astype(jnp.float32)
    lower, upper = jnp.where(first, own, other), jnp.where(first, other, own)
    for block in range(blocks):
        here = slice(block * share, (block + 1) * share)
        wide_ref[block, 0:share] = lower[here]
        wide_ref[block, share:capacity] = upper[here]
    out_ref[...] = wide_ref[...].astype(out_ref.dtype)


def unfold(own, other, blocks, capacity):
    shape = (blocks, capacity, own.shape[1])
    return pl.pallas_call(
        unfold_kernel,
        out_shape=jax.ShapeDtypeStruct(shape, own.dtype),
        scratch_shapes=[pltpu.VMEM(shape, jnp.float32)],
        compiler_params=vmem(8),
        name="unfold",
    )(own, other)


def combine_kernel(state_ref, slot_ref, weight_ref, returned_ref, out_ref, rows_ref):
    blocks, capacity, _ = returned_ref.shape
    pitch = padded(capacity)
    rows_ref[...] = jnp.zeros_like(rows_ref)
    for block in range(blocks):
        rows_ref[block * pitch : block * pitch + capacity] = returned_ref[block].astype(jnp.float32)
    rows = rows_ref[...].astype(jnp.bfloat16)
    place = lax.broadcasted_iota(jnp.int32, (state_ref.shape[0], blocks * pitch), 1)
    total = jnp.zeros(out_ref.shape, jnp.float32)
    for choice in range(slot_ref.shape[1]):
        pick = jnp.where(place == slot_ref[:, choice : choice + 1], 1.0, 0.0).astype(jnp.bfloat16)
        picked = jnp.dot(pick, rows, preferred_element_type=jnp.float32)
        total += weight_ref[:, choice : choice + 1] * picked
    out_ref[...] = (state_ref[...].astype(jnp.float32) + total).astype(out_ref.dtype)


def combine(state, slots, weights, returned):
    blocks, capacity, width = returned.shape
    return pl.pallas_call(
        combine_kernel,
        out_shape=jax.ShapeDtypeStruct(state.shape, jnp.bfloat16),
        scratch_shapes=[pltpu.VMEM((blocks * padded(capacity), width), jnp.float32)],
        compiler_params=vmem(12),
        name="combine",
    )(state, slots, weights, returned)


def route_weights(routes, group_logits, expert_scores, per_group):
    raised = jnp.exp(group_logits)
    group_prob = raised / jnp.sum(raised, axis=1, keepdims=True)
    owning_group = routes // per_group
    groups_iota = jnp.arange(group_logits.shape[1], dtype=jnp.int32)
    picked = jnp.sum(
        jnp.where(owning_group[:, :, None] == groups_iota[None, None, :], group_prob[:, None, :], 0.0),
        axis=2,
    )
    lifted = jnp.exp(expert_scores)
    return picked * lifted / jnp.sum(lifted, axis=1, keepdims=True)


def to_travel(values):
    wide = values.astype(jnp.float32)
    root = jnp.sqrt(jnp.abs(wide))
    return jnp.where(wide < 0, -root, root).astype(jnp.float16)


def from_travel(roots):
    wide = roots.astype(jnp.float32)
    return (wide * jnp.abs(wide)).astype(jnp.bfloat16)


def to_line(values):
    return from_travel(lax.all_gather(to_travel(values), LINE, axis=0, tiled=False))


def swap(values):
    return lax.ppermute(values, "core", [(0, 1), (1, 0)])


def gain_rows(gain):
    row = lax.broadcasted_iota(jnp.int32, (GAIN_ROWS, gain.shape[0]), 0)
    rows, rest = jnp.zeros(row.shape, jnp.float32), gain[None, :]
    for k in range(3):
        head = lax.reduce_precision(rest, 8, 7)
        rows = jnp.where(row == k, head, rows)
        rest = rest - head
    return rows.astype(jnp.bfloat16)


def per_device(
    pool_input,
    pool_gate,
    pool_mix,
    pool_scale,
    out_proj,
    residual,
    norm_gain,
    routes,
    group_logits,
    expert_scores,
    w_gate,
    w_up,
    w_down,
):
    channels, length = pool_input.shape
    blocks = lax.axis_size("sp")
    experts = blocks * w_gate.shape[0]
    capacity = 3 * routes.shape[1] * length // (2 * experts)
    scale, quarter = lax.axis_index("tg"), lax.axis_index(SCALE)
    core = lax.axis_index("core")
    own_first = (scale * lax.axis_size(SCALE) + quarter) * channels
    edge = lax.ppermute(
        pool_input[:, length - SPAN :], "sp", [(i, i + 1) for i in range(blocks - 1)]
    )
    slots = slot_table(routes.T, experts, padded(capacity))
    gains = gain_rows(norm_gain)
    pooled = pool(edge, pool_input, gains)
    group = lax.all_gather(pooled, SCALE, axis=0, tiled=True)
    mix = lax.dynamic_slice(
        pool_mix, (scale, 0, quarter * channels), (1, pool_mix.shape[1], channels)
    )[0]
    mixed = lax.dot_general(mix, group[:, :length], (((0,), (0,)), ((), ())), preferred_element_type=jnp.float32)
    other_gains = lax.dynamic_slice(group, ((quarter + 1 - 2 * core) * channels, length), (GAIN_ROWS, SPAN))
    own_scale = lax.dynamic_slice(pool_scale, (own_first,), (channels,))
    branch = (jax.nn.sigmoid(pool_gate.astype(jnp.float32)) * mixed * own_scale[:, None]).astype(jnp.bfloat16)
    branches = lax.all_gather(branch, TP, axis=0, tiled=True)
    product = lax.dot_general(
        branches, out_proj, (((0,), (0,)), ((), ())), preferred_element_type=jnp.float32
    )
    state = (residual.astype(jnp.float32) + product).astype(jnp.bfloat16)

    other_state, other_gains = lax.optimization_barrier((swap(state), other_gains))
    sent = dispatch(state, other_state, slots, blocks, capacity)
    w_gate, w_up, w_down = w_gate[0], w_up[0], w_down[0]
    other_gate, other_up, other_down = swap(w_gate), swap(w_up), swap(w_down)
    arrived = lax.all_to_all(sent, "sp", split_axis=0, concat_axis=0, tiled=True)
    everyone = to_line(compact(arrived, gains, other_gains))
    activated = hidden(everyone, w_gate, w_up, other_gate, other_up)
    own_result, other_result = down(to_line(activated), w_down, other_down)
    result = unfold(own_result, swap(other_result), blocks, capacity)
    result, routes, group_logits, expert_scores = lax.optimization_barrier(
        (result, routes, group_logits, expert_scores)
    )
    weights = route_weights(routes, group_logits, expert_scores, experts // group_logits.shape[1])
    returned = lax.all_to_all(result, "sp", split_axis=0, concat_axis=0, tiled=True)
    return combine(state, slots.T, weights, returned)


def solution(mesh):
    fine = Mesh(mesh.devices.reshape(mesh.devices.shape[0], 4, -1, 2), ("sp", *TP))
    placed = (
        P(TP, "sp"),
        P(TP, "sp"),
        P(),
        P(),
        P(None, TP),
        P("sp", TP),
        P(TP),
        P("sp", None),
        P("sp", None),
        P("sp", None),
        P("sp", None, TP),
        P("sp", None, TP),
        P("sp", None, TP),
    )
    return jax.shard_map(
        per_device, mesh=fine, in_specs=placed, out_specs=P("sp", TP), check_vma=False
    )
```

```python
import jax
import jax.numpy as jnp
from jax import lax
from jax.experimental import pallas as pl
from jax.experimental.pallas import tpu as pltpu
from jax.sharding import Mesh, PartitionSpec as P

SPAN = 128
GAIN_ROWS = 16
TOGETHER = 2
AHEAD = 2
DOWN_AHEAD = 4
HIDDEN_MIB = 20
DOWN_MIB = 16
ROWS = 288
epsilon = 1e-06

LINE = ("tg", "yl")
SCALE = ("yl", "core")
TP = (*LINE, "core")


def vmem(mib):
    return pltpu.CompilerParams(vmem_limit_bytes=mib << 20)


def padded(rows):
    return -(-rows // 8) * 8


def pool_kernel(edge_ref, own_ref, gain_ref, out_ref):
    length = own_ref.shape[1]
    scale = lax.axis_index("tg")
    first = lax.axis_index("sp") * length
    own = own_ref[...].astype(jnp.float32)
    layered = jnp.concatenate([edge_ref[...].astype(jnp.float32), own], axis=1)
    chosen = None
    stride = 1
    for octave in range(4):
        layered = layered + pltpu.roll(layered, stride, 1)
        stride *= 2
        chosen = layered if chosen is None else jnp.where(scale >= octave, layered, chosen)
    window = jnp.left_shift(2, scale)
    position = first + 1 + lax.broadcasted_iota(jnp.int32, own.shape, 1)
    counted = jnp.minimum(position, window).astype(jnp.float32)
    pooled = chosen[:, SPAN : SPAN + length] / counted - own
    out_ref[:, :length] = pooled.astype(out_ref.dtype)
    out_ref[:, length:] = jnp.zeros((own.shape[0], SPAN), out_ref.dtype)
    out_ref[0:GAIN_ROWS, length:] = gain_ref[...]


def pool(edge, own, gains):
    channels, length = own.shape
    return pl.pallas_call(
        pool_kernel,
        out_shape=jax.ShapeDtypeStruct((channels, length + SPAN), jnp.bfloat16),
        compiler_params=vmem(4),
        name="pool",
    )(edge, own, gains)


def slot_kernel(experts, pitch, routes_ref, out_ref):
    choices, length = routes_ref.shape
    number = lax.broadcasted_iota(jnp.int32, (experts, length), 0)
    named = [(number == routes_ref[k : k + 1, :]).astype(jnp.float32) for k in range(choices)]
    earlier = lax.broadcasted_iota(jnp.int32, (length, length), 0) < lax.broadcasted_iota(
        jnp.int32, (length, length), 1
    )
    before = jnp.dot(
        sum(named).astype(jnp.bfloat16),
        jnp.where(earlier, 1.0, 0.0).astype(jnp.bfloat16),
        preferred_element_type=jnp.float32,
    )
    for k in range(choices):
        rank = jnp.sum(before * named[k], axis=0, keepdims=True).astype(jnp.int32)
        out_ref[k : k + 1, :] = routes_ref[k : k + 1, :] * pitch + rank


def slot_table(routes, experts, pitch):
    def kernel(routes_ref, out_ref):
        slot_kernel(experts, pitch, routes_ref, out_ref)

    return pl.pallas_call(
        kernel,
        out_shape=jax.ShapeDtypeStruct(routes.shape, jnp.int32),
        compiler_params=vmem(8),
        name="slots",
    )(routes)


def dispatch_kernel(pitch, own_ref, other_ref, slot_ref, out_ref):
    blocks, share, _ = out_ref.shape
    core, stride = lax.axis_index("core"), padded(share)
    first = core == 0
    own, other = own_ref[...].astype(jnp.float32), other_ref[...].astype(jnp.float32)
    state = jnp.concatenate([jnp.where(first, own, other), jnp.where(first, other, own)], axis=1)
    count = lax.broadcasted_iota(jnp.int32, (stride, own_ref.shape[0]), 0) + core * share
    place = jnp.concatenate([count + block * pitch for block in range(blocks)], axis=0)
    chosen = place == slot_ref[0:1, :]
    for k in range(1, slot_ref.shape[0]):
        chosen = chosen | (place == slot_ref[k : k + 1, :])
    spread = jnp.where(chosen, 1.0, 0.0).astype(jnp.bfloat16)
    rows = jnp.dot(spread, state.astype(jnp.bfloat16), preferred_element_type=jnp.float32)
    for block in range(blocks):
        out_ref[block] = rows[block * stride : block * stride + share].astype(out_ref.dtype)


def dispatch(own, other, slots, blocks, capacity):
    def kernel(*refs):
        dispatch_kernel(padded(capacity), *refs)

    return pl.pallas_call(
        kernel,
        out_shape=jax.ShapeDtypeStruct((blocks, capacity // 2, 2 * own.shape[1]), jnp.bfloat16),
        compiler_params=vmem(12),
        name="dispatch",
    )(own, other, slots)


def compact_kernel(arrived_ref, own_ref, other_ref, out_ref, rows_ref):
    blocks, share, width = arrived_ref.shape
    rows = blocks * share
    first = lax.axis_index("core") == 0
    for block in range(blocks):
        rows_ref[block * share : (block + 1) * share] = arrived_ref[block].astype(jnp.float32)
    own, other = own_ref[...].astype(jnp.float32), other_ref[...].astype(jnp.float32)
    rows_ref[rows:, : width // 2] = jnp.where(first, own, other)
    rows_ref[rows:, width // 2 :] = jnp.where(first, other, own)
    out_ref[...] = rows_ref[...].astype(out_ref.dtype)


def compact(arrived, own_gains, other_gains):
    shape = (arrived.shape[0] * arrived.shape[1] + GAIN_ROWS, arrived.shape[2])
    return pl.pallas_call(
        compact_kernel,
        out_shape=jax.ShapeDtypeStruct(shape, jnp.bfloat16),
        scratch_shapes=[pltpu.VMEM(shape, jnp.float32)],
        compiler_params=vmem(8),
        name="compact",
    )(arrived, own_gains, other_gains)


def tiles(rows, limit):
    size = -(-rows // -(-rows // limit) // 16) * 16
    return [(first, min(size, rows - first)) for first in range(0, rows, size)]


def begin_ahead(copies, ahead):
    for copy in sum(copies[:ahead], []):
        copy.start()


def turn_over(copies, chunk, ahead):
    for copy in copies[chunk]:
        copy.wait()
    for copy in sum(copies[chunk + ahead : chunk + ahead + 1], []):
        copy.start()


def hidden_kernel(x_ref, gate_ref, up_ref, gate2_hbm, up2_hbm, out_ref, gate2_ref, up2_ref, squares_ref, *refs):
    sums, w_sems = refs[:4], refs[4]
    parts, rows, width = x_ref.shape
    rows -= GAIN_ROWS
    units = gate_ref.shape[1]
    depth = TOGETHER * width
    chunks = parts // TOGETHER
    copies = []
    for chunk in range(chunks):
        deep = pl.ds(chunk * depth, depth)
        copies.append(
            [
                pltpu.make_async_copy(hbm.at[deep], ref.at[deep], w_sems.at[chunk, k])
                for k, (hbm, ref) in enumerate(((gate2_hbm, gate2_ref), (up2_hbm, up2_ref)))
            ]
        )
    begin_ahead(copies, AHEAD)
    for chunk in range(chunks):
        turn_over(copies, chunk, AHEAD)
        mine = range(chunk * TOGETHER, (chunk + 1) * TOGETHER)
        deep = pl.ds(chunk * depth, depth)
        gains = []
        for part in mine:
            extra = x_ref[part, pl.ds(rows, GAIN_ROWS), :].astype(jnp.float32)
            gains.append(extra[0:1] + extra[1:2] + extra[2:3])
        for first, count in tiles(rows, ROWS):
            here = pl.ds(first, count)
            squares, scaled = None, []
            for part, gain in zip(mine, gains):
                state = x_ref[part, here, :].astype(jnp.float32)
                squares = state * state if squares is None else squares + state * state
                scaled.append((state * gain).astype(jnp.bfloat16))
            rows_in = jnp.concatenate(scaled, axis=1)
            if chunk == 0:
                squares_ref[here, :] = squares
            else:
                squares_ref[here, :] += squares
            for total_ref, weight_ref in zip(sums, (gate_ref, up_ref, gate2_ref, up2_ref)):
                product = jnp.dot(rows_in, weight_ref[deep, :], preferred_element_type=jnp.float32)
                if chunk == 0:
                    total_ref[here, :] = product
                else:
                    total_ref[here, :] += product
    lower = lax.axis_index("core") == 0
    for first, count in tiles(rows, ROWS):
        here = pl.ds(first, count)
        mean = jnp.sum(squares_ref[here, :], axis=1, keepdims=True) / (parts * width)
        factor = lax.rsqrt(mean + epsilon)
        gate, up, gate2, up2 = [total_ref[here, :] * factor for total_ref in sums]
        own, other = jax.nn.silu(gate) * up, jax.nn.silu(gate2) * up2
        out_ref[here, :units] = jnp.where(lower, own, other).astype(out_ref.dtype)
        out_ref[here, units:] = jnp.where(lower, other, own).astype(out_ref.dtype)


def hidden(everyone, w_gate, w_up, other_gate, other_up):
    parts, extended, width = everyone.shape
    rows, units = extended - GAIN_ROWS, w_gate.shape[1]
    hbm, near = pl.BlockSpec(memory_space=pltpu.HBM), pl.BlockSpec(memory_space=pltpu.VMEM)
    return pl.pallas_call(
        hidden_kernel,
        out_shape=jax.ShapeDtypeStruct((rows, 2 * units), jnp.bfloat16),
        in_specs=[near, near, near, hbm, hbm],
        scratch_shapes=[
            pltpu.VMEM(w_gate.shape, w_gate.dtype),
            pltpu.VMEM(w_up.shape, w_up.dtype),
            pltpu.VMEM((rows, width), jnp.float32),
            *[pltpu.VMEM((rows, units), jnp.float32)] * 4,
            pltpu.SemaphoreType.DMA((parts // TOGETHER, 2)),
        ],
        compiler_params=vmem(HIDDEN_MIB),
        name="hidden",
    )(everyone, w_gate, w_up, other_gate, other_up)


def down_kernel(u_ref, own_hbm, other_hbm, own_out, other_out, own_ref, other_ref, total_ref, w_sems):
    parts, rows, units = u_ref.shape
    width = own_ref.shape[1]
    copies = []
    for part in range(parts):
        deep = pl.ds(part * units, units)
        copies.append(
            [
                pltpu.make_async_copy(own_hbm.at[deep], own_ref.at[deep], w_sems.at[part, 0]),
                pltpu.make_async_copy(other_hbm.at[deep], other_ref.at[deep], w_sems.at[part, 1]),
            ]
        )
    begin_ahead(copies, DOWN_AHEAD)
    for part in range(parts):
        turn_over(copies, part, DOWN_AHEAD)
        deep = pl.ds(part * units, units)
        columns = jnp.concatenate([own_ref[deep, :], other_ref[deep, :]], axis=1)
        for first, count in tiles(rows, ROWS):
            here = pl.ds(first, count)
            product = jnp.dot(u_ref[part, here, :], columns, preferred_element_type=jnp.float32)
            if part == 0:
                total_ref[here, :] = product
            else:
                total_ref[here, :] += product
    own_out[...] = total_ref[:, :width].astype(own_out.dtype)
    other_out[...] = total_ref[:, width:].astype(other_out.dtype)


def down(everyone, own, other):
    parts, rows, units = everyone.shape
    width = own.shape[1]
    half = jax.ShapeDtypeStruct((rows, width), jnp.bfloat16)
    hbm, near = pl.BlockSpec(memory_space=pltpu.HBM), pl.BlockSpec(memory_space=pltpu.VMEM)
    return pl.pallas_call(
        down_kernel,
        out_shape=[half, half],
        in_specs=[near, hbm, hbm],
        scratch_shapes=[
            pltpu.VMEM(own.shape, own.dtype),
            pltpu.VMEM(other.shape, other.dtype),
            pltpu.VMEM((rows, 2 * width), jnp.float32),
            pltpu.SemaphoreType.DMA((parts, 2)),
        ],
        compiler_params=vmem(DOWN_MIB),
        name="down",
    )(everyone, own, other)


def unfold_kernel(own_ref, other_ref, out_ref, wide_ref):
    blocks, capacity, _ = out_ref.shape
    share = capacity // 2
    first = lax.axis_index("core") == 0
    own, other = own_ref[...].astype(jnp.float32), other_ref[...].astype(jnp.float32)
    lower, upper = jnp.where(first, own, other), jnp.where(first, other, own)
    for block in range(blocks):
        here = slice(block * share, (block + 1) * share)
        wide_ref[block, 0:share] = lower[here]
        wide_ref[block, share:capacity] = upper[here]
    out_ref[...] = wide_ref[...].astype(out_ref.dtype)


def unfold(own, other, blocks, capacity):
    shape = (blocks, capacity, own.shape[1])
    return pl.pallas_call(
        unfold_kernel,
        out_shape=jax.ShapeDtypeStruct(shape, own.dtype),
        scratch_shapes=[pltpu.VMEM(shape, jnp.float32)],
        compiler_params=vmem(8),
        name="unfold",
    )(own, other)


def combine_kernel(state_ref, slot_ref, weight_ref, returned_ref, out_ref, rows_ref):
    blocks, capacity, _ = returned_ref.shape
    pitch = padded(capacity)
    rows_ref[...] = jnp.zeros_like(rows_ref)
    for block in range(blocks):
        rows_ref[block * pitch : block * pitch + capacity] = returned_ref[block].astype(jnp.float32)
    rows = rows_ref[...].astype(jnp.bfloat16)
    place = lax.broadcasted_iota(jnp.int32, (state_ref.shape[0], blocks * pitch), 1)
    total = jnp.zeros(out_ref.shape, jnp.float32)
    for choice in range(slot_ref.shape[1]):
        pick = jnp.where(place == slot_ref[:, choice : choice + 1], 1.0, 0.0).astype(jnp.bfloat16)
        picked = jnp.dot(pick, rows, preferred_element_type=jnp.float32)
        total += weight_ref[:, choice : choice + 1] * picked
    out_ref[...] = (state_ref[...].astype(jnp.float32) + total).astype(out_ref.dtype)


def combine(state, slots, weights, returned):
    blocks, capacity, width = returned.shape
    return pl.pallas_call(
        combine_kernel,
        out_shape=jax.ShapeDtypeStruct(state.shape, jnp.bfloat16),
        scratch_shapes=[pltpu.VMEM((blocks * padded(capacity), width), jnp.float32)],
        compiler_params=vmem(12),
        name="combine",
    )(state, slots, weights, returned)


def route_weights(routes, group_logits, expert_scores, per_group):
    raised = jnp.exp(group_logits)
    group_prob = raised / jnp.sum(raised, axis=1, keepdims=True)
    owning_group = routes // per_group
    groups_iota = jnp.arange(group_logits.shape[1], dtype=jnp.int32)
    picked = jnp.sum(
        jnp.where(owning_group[:, :, None] == groups_iota[None, None, :], group_prob[:, None, :], 0.0),
        axis=2,
    )
    lifted = jnp.exp(expert_scores)
    return picked * lifted / jnp.sum(lifted, axis=1, keepdims=True)


def to_travel(values):
    wide = values.astype(jnp.float32)
    root = jnp.sqrt(jnp.abs(wide))
    return jnp.where(wide < 0, -root, root).astype(jnp.float16)


def from_travel(roots):
    wide = roots.astype(jnp.float32)
    return (wide * jnp.abs(wide)).astype(jnp.bfloat16)


def to_line(values):
    return from_travel(lax.all_gather(to_travel(values), LINE, axis=0, tiled=False))


def swap(values):
    return lax.ppermute(values, "core", [(0, 1), (1, 0)])


def gain_rows(gain):
    row = lax.broadcasted_iota(jnp.int32, (GAIN_ROWS, gain.shape[0]), 0)
    rows, rest = jnp.zeros(row.shape, jnp.float32), gain[None, :]
    for k in range(3):
        head = lax.reduce_precision(rest, 8, 7)
        rows = jnp.where(row == k, head, rows)
        rest = rest - head
    return rows.astype(jnp.bfloat16)


def per_device(
    pool_input,
    pool_gate,
    pool_mix,
    pool_scale,
    out_proj,
    residual,
    norm_gain,
    routes,
    group_logits,
    expert_scores,
    w_gate,
    w_up,
    w_down,
):
    channels, length = pool_input.shape
    blocks = lax.axis_size("sp")
    experts = blocks * w_gate.shape[0]
    capacity = 3 * routes.shape[1] * length // (2 * experts)
    scale, quarter = lax.axis_index("tg"), lax.axis_index(SCALE)
    core = lax.axis_index("core")
    own_first = (scale * lax.axis_size(SCALE) + quarter) * channels
    edge = lax.ppermute(
        pool_input[:, length - SPAN :], "sp", [(i, i + 1) for i in range(blocks - 1)]
    )
    slots = slot_table(routes.T, experts, padded(capacity))
    gains = gain_rows(norm_gain)
    own, opened = lax.optimization_barrier(
        (pool_input.astype(jnp.float32), jax.nn.sigmoid(pool_gate.astype(jnp.float32)))
    )
    pooled = pool(edge, own, gains)
    group = lax.all_gather(pooled, SCALE, axis=0, tiled=True)
    mix = lax.dynamic_slice(
        pool_mix, (scale, 0, quarter * channels), (1, pool_mix.shape[1], channels)
    )[0]
    mixed = lax.dot_general(mix, group[:, :length], (((0,), (0,)), ((), ())), preferred_element_type=jnp.float32)
    other_gains = lax.dynamic_slice(group, ((quarter + 1 - 2 * core) * channels, length), (GAIN_ROWS, SPAN))
    own_scale = lax.dynamic_slice(pool_scale, (own_first,), (channels,))
    branch = (opened * mixed * own_scale[:, None]).astype(jnp.bfloat16)
    branches = lax.all_gather(branch, TP, axis=0, tiled=True)
    product = lax.dot_general(
        branches, out_proj, (((0,), (0,)), ((), ())), preferred_element_type=jnp.float32
    )
    state = (residual.astype(jnp.float32) + product).astype(jnp.bfloat16)

    other_state, other_gains = lax.optimization_barrier((swap(state), other_gains))
    sent = dispatch(state, other_state, slots, blocks, capacity)
    w_gate, w_up, w_down = w_gate[0], w_up[0], w_down[0]
    other_gate, other_up, other_down = swap(w_gate), swap(w_up), swap(w_down)
    arrived = lax.all_to_all(sent, "sp", split_axis=0, concat_axis=0, tiled=True)
    everyone = to_line(compact(arrived, gains, other_gains))
    activated = hidden(everyone, w_gate, w_up, other_gate, other_up)
    own_result, other_result = down(to_line(activated), w_down, other_down)
    result = unfold(own_result, swap(other_result), blocks, capacity)
    result, routes, group_logits, expert_scores = lax.optimization_barrier(
        (result, routes, group_logits, expert_scores)
    )
    weights = route_weights(routes, group_logits, expert_scores, experts // group_logits.shape[1])
    returned = lax.all_to_all(result, "sp", split_axis=0, concat_axis=0, tiled=True)
    return combine(state, slots.T, weights, returned)


def solution(mesh):
    fine = Mesh(mesh.devices.reshape(mesh.devices.shape[0], 4, -1, 2), ("sp", *TP))
    placed = (
        P(TP, "sp"),
        P(TP, "sp"),
        P(),
        P(),
        P(None, TP),
        P("sp", TP),
        P(TP),
        P("sp", None),
        P("sp", None),
        P("sp", None),
        P("sp", None, TP),
        P("sp", None, TP),
        P("sp", None, TP),
    )
    return jax.shard_map(
        per_device, mesh=fine, in_specs=placed, out_specs=P("sp", TP), check_vma=False
    )
```
